32 devices in a mesh: sp: 4 (over y, x), tp: 8 (over z, core).
Axes of the slice: x: 2, y: 2, z: 4, core: 2. Of those that a mesh axis runs over, the one named last changes fastest.
Arguments:
- skip_stream_entry: bfloat16 [2048, 2048], P(('sp', 'tp')), may hold values from -6 to 6
- result_switch_mapped: bfloat16 [2048, 4096], P('sp', 'tp'), may hold values from -6 to 6
- channel_feed_mapped: bfloat16 [2048, 4096], P('sp', 'tp'), may hold values from -6 to 6
- write_coefficient_mapped: bfloat16 [2048, 2048], P('sp', 'tp'), may hold values from -6 to 6
- emission_coefficient_mapped: bfloat16 [2048, 2048], P('sp', 'tp'), may hold values from -6 to 6
- channel_feed_taps: bfloat16 [5, 4096], P(None, 'tp'), may hold values from -2.5 to 2.5
- write_coefficient_taps: bfloat16 [5, 2048], P(None, 'tp'), may hold values from -2.5 to 2.5
- emission_coefficient_taps: bfloat16 [5, 2048], P(None, 'tp'), may hold values from -2.5 to 2.5
- raw_increments: bfloat16 [2, 64, 2048], P(None, 'tp', 'sp'), may hold values from -6 to 6
- channel_log_fade_speed: float32 [2, 64], P(None, 'tp'), may hold values from -20 to 0
- extra_log_fade: float32 [2, 64, 2048], P(None, 'tp', 'sp'), may hold values from -1 to 0
- cluster_scaling_factor: float32 [4096], P('tp'), may hold values from 0.1 to 1.9
- blend_result_matrix: bfloat16 [4096, 2048], P('tp'), may hold values from -0.09375 to 0.09375
- routing_scaling_factor: float32 [2048], replicated, may hold values from 0.1 to 1.9
- specialist_switch_matrix: bfloat16 [8, 2048, 4096], P('sp', None, 'tp'), may hold values from -0.125 to 0.125
- specialist_widen_matrix: bfloat16 [8, 2048, 4096], P('sp', None, 'tp'), may hold values from -0.125 to 0.125
- specialist_contract_matrix: bfloat16 [8, 4096, 2048], P('sp', 'tp'), may hold values from -0.1875 to 0.1875
- picked_specialists: int32 [2048, 2], P(('sp', 'tp')), may hold values from 0 to 7, all different within a row; in each aligned block of 64 rows (0 to 63, 64 to 127, ...) at most 24 rows name the same one
- router_affinities: float32 [2048, 2], P(('sp', 'tp')), may hold values from 0.1 to 1
Outputs:
- result: bfloat16 [2048, 2048], P(('sp', 'tp'))
The draws below stay inside these ranges and needn't reach their ends.
Inputs may be any that keep to these rules, and one draw needn't show every extreme that they name: `picked_specialists`: each row names 2 different experts. Within the rows of one device (aligned blocks of 64 rows) no expert is named more than 24 times, a bound that some block reaches.
All inputs are finite; a program needn't handle non-finite values.
Results may differ from the reference program's by a relative error of at most 0.02.
Values may be sent and summed in bfloat16 or wider, within the bound.
A program may use at most 64 MiB of HBM per device.

```python
import math
import jax
import jax.numpy as jnp
import numpy as np
from jax import lax

WIDTH = 2048
HEADS = 64
HEAD_DIM = 64
GROUPS = 16
STATE = 128
EXPERT_FF = 4096
CONV_W = 5
BLOCK = 128
TOP = 2
SEQ_DEV = 512
INNER = 4096
SERIES_ITEMS = 2048
ROWS_DEV = 64
EXPERTS = 8
CAPACITY = 24
N_SP = 4
N_TP = 8


def draw_raw_increments(key, part):
    first_key, second_key = jax.random.split(key)
    noise = 0.7 * jax.random.normal(second_key, (2, HEADS, SERIES_ITEMS), jnp.float32)
    shifts = jax.random.uniform(first_key, (2, HEADS, SERIES_ITEMS // SEQ_DEV), jnp.float32, -1.5, 1.0)
    return (noise + jnp.repeat(shifts, SEQ_DEV, axis=2)).astype(jnp.bfloat16)


def draw_channel_log_fade_speed(key, part):
    coin_key, slow_key, fast_key = jax.random.split(key, 3)
    share = 0.5
    slow = jnp.log(jax.random.uniform(slow_key, (2, HEADS), jnp.float32, 0.1, 0.4) / SERIES_ITEMS)
    fast = jnp.log(jax.random.uniform(fast_key, (2, HEADS), jnp.float32, 0.05, 0.12))
    return jnp.where(jax.random.uniform(coin_key, (2, HEADS), jnp.float32) < share, slow, fast)


def draw_extra_log_fade(key, part):
    place_key, depth_key = jax.random.split(key)
    third = SERIES_ITEMS // 3
    offsets = jnp.arange(3, dtype=jnp.int32) * third
    places = offsets[None, None, :] + jax.random.randint(place_key, (2, HEADS, 3), 0, third, dtype=jnp.int32)
    depths = jnp.log(jax.random.uniform(depth_key, (2, HEADS, 3), jnp.float32, 0.5, 0.8))
    positions = jnp.arange(SERIES_ITEMS, dtype=jnp.int32)
    landed = positions[None, None, None, :] == places[..., None]
    return jnp.sum(jnp.where(landed, depths[..., None], 0.0), axis=2)


def level_of(rng, dims, cuts, least, largest):
    level, own = 1.0, jax.random.fold_in(rng, 6)
    for position, blocks in cuts:
        heights = jnp.exp(jax.random.uniform(jax.random.fold_in(own, position), (blocks,), jnp.float32, least / len(cuts), largest / len(cuts)))
        level = level * jnp.repeat(heights, dims[position] // blocks).reshape([-1 if axis == position else 1 for axis in range(len(dims))])
    return level


def shared_out(stream_key, own, number, rows, number_of, top, bound, skew):
    order = jax.random.permutation(stream_key, number_of)
    heavy_load, common = load_shares(number_of, rows * top, bound, skew, True), load_shares(number_of, rows * top, bound, skew, False)
    places = jnp.arange(number_of)

    def named(lengths, offset_by):
        used = int((lengths > 0).sum())
        fixed = max(1, used // 4)
        moved = fixed + (places - fixed + offset_by * (used - fixed)) % max(1, number_of - fixed)
        return jnp.zeros((number_of,), jnp.int32).at[order[jnp.where(places < fixed, places, moved)]].set(jnp.asarray(lengths, jnp.int32))

    lengths = jnp.where(number % 4 == 0, named(heavy_load, number // 4), named(common, number - number // 4 - 1))
    mixed = jax.random.permutation(jax.random.fold_in(own, 3), number_of)
    source_of, sink = mixed[0:number_of // 2 * 2:2], mixed[1:number_of // 2 * 2:2]
    room = jnp.minimum(lengths[source_of] - 1, bound - lengths[sink]) // 2
    room = jnp.where((source_of == order[0]) | (sink == order[0]) | (lengths[sink] == 0), 0, jnp.maximum(room, 0))
    moved = jax.random.randint(jax.random.fold_in(own, 4), (number_of // 2,), 0, 1 << 20) % (room + 1)
    lengths = lengths.at[source_of].add(-moved).at[sink].add(moved)
    members = jnp.searchsorted(jnp.cumsum(lengths), jnp.arange(rows * top), side="right").astype(jnp.int32)
    table = members.reshape(top, rows).T
    table = table[jax.random.permutation(jax.random.fold_in(own, 1), rows)]
    offset_by = jax.random.randint(jax.random.fold_in(own, 2), (rows, 1), 0, top)
    return jnp.take_along_axis(table, (jnp.arange(top)[None, :] + offset_by) % top, axis=1)


def load_shares(number_of, total, most, lean, full):
    weights = [(1 << 20) // math.isqrt(rank ** lean) + 1 for rank in range(1, number_of + 1)]
    largest = most if full else min(most, max(-(-total // number_of), total * weights[0] // sum(weights)))
    least = 1 if total - largest >= number_of - 1 else 0
    holding, spare = [largest] + [least] * (number_of - 1), total - largest - least * (number_of - 1)
    while spare > 0:
        free = [i for i in range(1, number_of) if holding[i] < largest] or [i for i in range(1, number_of) if holding[i] < most]
        whole, left = sum([weights[i] for i in free]), spare
        for i in free:
            addition = min(most - holding[i], max(1, left * weights[i] // whole), spare)
            holding[i] = holding[i] + addition
            spare = spare - addition
    return np.array(holding)


def scatter_about(rng, shape, scale, bound, cuts=(), kind=jnp.bfloat16):
    entries = scale * jax.random.normal(rng, shape, jnp.float32)
    if cuts:
        entries = entries * level_of(rng, shape, cuts, -0.22, 0.18)
    return jnp.clip(entries, -bound, bound).astype(kind)


def setup_inputs(seed: int = 0) -> dict:
    splits = jax.random.split(jax.random.key(seed), 20)
    skip_stream_entry = scatter_about(splits[0], (SERIES_ITEMS, WIDTH), 1.0, 6.0, ((0, 32),))
    result_switch_mapped = scatter_about(splits[1], (SERIES_ITEMS, INNER), 1.0, 6.0, ((0, 4), (1, 8)))
    channel_feed_mapped = scatter_about(splits[2], (SERIES_ITEMS, INNER), 1.0, 6.0, ((0, 4), (1, 8)))
    write_coefficient_mapped = scatter_about(splits[3], (SERIES_ITEMS, GROUPS * STATE), 1.0, 6.0, ((0, 4), (1, 8)))
    emission_coefficient_mapped = scatter_about(splits[4], (SERIES_ITEMS, GROUPS * STATE), 1.0, 6.0, ((0, 4), (1, 8)))
    channel_feed_taps = scatter_about(splits[5], (CONV_W, INNER), CONV_W ** -0.5, 2.5, ((1, 8),))
    write_coefficient_taps = scatter_about(splits[6], (CONV_W, GROUPS * STATE), CONV_W ** -0.5, 2.5, ((1, 8),))
    emission_coefficient_taps = scatter_about(splits[7], (CONV_W, GROUPS * STATE), CONV_W ** -0.5, 2.5, ((1, 8),))
    raw_increments = draw_raw_increments(jax.random.fold_in(splits[19], 71), 0)
    channel_log_fade_speed = draw_channel_log_fade_speed(jax.random.fold_in(splits[19], 71), 0)
    extra_log_fade = draw_extra_log_fade(jax.random.fold_in(splits[19], 71), 0)
    cluster_scaling_factor = jnp.clip(1.0 + 0.18 * jax.random.normal(splits[11], (INNER,), jnp.float32), 0.1, 1.9)
    blend_result_matrix = scatter_about(splits[12], (INNER, WIDTH), INNER ** -0.5, 0.09375, ((0, 8),))
    routing_scaling_factor = jnp.clip(1.0 + 0.18 * jax.random.normal(splits[13], (WIDTH,), jnp.float32), 0.1, 1.9)
    specialist_switch_matrix = scatter_about(splits[14], (EXPERTS, WIDTH, EXPERT_FF), WIDTH ** -0.5, 0.125, ((0, 4), (2, 8)))
    specialist_widen_matrix = scatter_about(splits[15], (EXPERTS, WIDTH, EXPERT_FF), WIDTH ** -0.5, 0.125, ((0, 4), (2, 8)))
    specialist_contract_matrix = scatter_about(splits[16], (EXPERTS, EXPERT_FF, WIDTH), (EXPERT_FF // 4) ** -0.5, 0.1875, ((0, 4), (1, 8)))
    picked_specialists_keys = jax.random.split(jax.random.fold_in(splits[17], 1), SERIES_ITEMS // ROWS_DEV)
    picked_specialists_turns = jax.random.permutation(jax.random.fold_in(splits[17], 3), SERIES_ITEMS // ROWS_DEV)
    picked_specialists = jax.vmap(lambda own, number: shared_out(jax.random.fold_in(splits[17], 2), own, number, ROWS_DEV, EXPERTS, TOP, CAPACITY, 1))(picked_specialists_keys, picked_specialists_turns).reshape((SERIES_ITEMS, TOP))
    router_affinities = jnp.clip(jnp.exp(math.log(1.0) - 2.3025851 * jax.random.uniform(splits[18], (SERIES_ITEMS, TOP), jnp.float32) ** level_of(splits[18], (SERIES_ITEMS, TOP), ((0, 32),), -0.2, 0.2)), 0.1, 1.0)
    return dict(skip_stream_entry=skip_stream_entry, result_switch_mapped=result_switch_mapped, channel_feed_mapped=channel_feed_mapped, write_coefficient_mapped=write_coefficient_mapped, emission_coefficient_mapped=emission_coefficient_mapped, channel_feed_taps=channel_feed_taps, write_coefficient_taps=write_coefficient_taps, emission_coefficient_taps=emission_coefficient_taps, raw_increments=raw_increments, channel_log_fade_speed=channel_log_fade_speed, extra_log_fade=extra_log_fade, cluster_scaling_factor=cluster_scaling_factor, blend_result_matrix=blend_result_matrix, routing_scaling_factor=routing_scaling_factor, specialist_switch_matrix=specialist_switch_matrix, specialist_widen_matrix=specialist_widen_matrix, specialist_contract_matrix=specialist_contract_matrix, picked_specialists=picked_specialists, router_affinities=router_affinities)


EPSILON = 1e-06
HIGHEST_MODE = lax.Precision.HIGHEST

def centred_conv(padded, weights, series_count):
    summed = jnp.zeros((series_count, padded.shape[1]), jnp.float32)
    for offset in range(weights.shape[0]):
        summed = summed + weights[offset].astype(jnp.float32) * padded[offset:offset + series_count].astype(jnp.float32)
    return jax.nn.silu(summed)

def local_sweep(inputs, entry_state, readout_state, log_fade_factor, softplus_increment):
    seq_len = inputs.shape[0]
    blocks = seq_len // BLOCK
    heads_here = log_fade_factor.shape[0]
    groups_here = entry_state.shape[1] // STATE
    per_group = heads_here // groups_here
    values = inputs.reshape(blocks, BLOCK, groups_here, per_group, HEAD_DIM)
    b_blocks = entry_state.reshape(blocks, BLOCK, groups_here, STATE)
    c_blocks = readout_state.reshape(blocks, BLOCK, groups_here, STATE)
    decay_blocks = log_fade_factor.reshape(groups_here, per_group, blocks, BLOCK)
    step_blocks = softplus_increment.reshape(groups_here, per_group, blocks, BLOCK)
    cumulative = jnp.cumsum(decay_blocks, axis=-1)
    group_inner = jnp.einsum('bign,bjgn->gbij', c_blocks, b_blocks, precision=HIGHEST_MODE)
    spread = cumulative[..., :, None] - cumulative[..., None, :]
    lower_tri = jnp.arange(BLOCK)[:, None] >= jnp.arange(BLOCK)[None, :]
    mixing = jnp.exp(jnp.where(lower_tri, spread, -jnp.inf)) * step_blocks[..., None, :] * group_inner[:, None]
    within = jnp.einsum('gkbij,bjgkp->bigkp', mixing, values, precision=HIGHEST_MODE)
    to_end = jnp.exp(cumulative[..., -1:] - cumulative) * step_blocks
    block_states = jnp.einsum('gkbj,bjgkp,bjgn->bgkpn', to_end, values, b_blocks, precision=HIGHEST_MODE)
    block_decay = cumulative[..., -1]

    def advance(carried, pieces):
        state_piece, decay_piece = pieces
        return (carried * jnp.exp(decay_piece)[..., None, None] + state_piece, carried)
    zero_state = jnp.zeros((groups_here, per_group, HEAD_DIM, STATE), jnp.float32)
    final_state, entering = lax.scan(advance, zero_state, (block_states, jnp.moveaxis(block_decay, -1, 0)))
    before = jnp.cumsum(block_decay, axis=-1) - block_decay
    return ((within, entering, cumulative, before, c_blocks), (lax.optimization_barrier(jnp.sum(block_decay, axis=-1)), final_state))

def finish_sweep(parts, carried):
    within, entering, cumulative, before, c_blocks = parts
    entering = entering + carried[None] * jnp.exp(jnp.moveaxis(before, -1, 0))[..., None, None]
    readout = jnp.einsum('bign,bgkpn->bigkp', c_blocks, entering, precision=HIGHEST_MODE)
    readout = readout * jnp.exp(jnp.transpose(cumulative, (2, 3, 0, 1)))[..., None]
    combined = within + readout
    return combined.reshape(combined.shape[0] * combined.shape[1], -1)

def blend_parts_list(channel_feed_bordered, write_coefficient_bordered, emission_coefficient_bordered, channel_feed_taps, write_coefficient_taps, emission_coefficient_taps, raw_increments, channel_log_fade_speed, extra_log_fade, series_count):
    inputs = centred_conv(channel_feed_bordered, channel_feed_taps, series_count)
    entry_state = centred_conv(write_coefficient_bordered, write_coefficient_taps, series_count)
    readout_state = centred_conv(emission_coefficient_bordered, emission_coefficient_taps, series_count)
    softplus_increment = jax.nn.softplus(raw_increments.astype(jnp.float32))
    log_fade_factor = -softplus_increment * jnp.exp(channel_log_fade_speed)[..., None] + extra_log_fade
    onward_pass = local_sweep(inputs, entry_state, readout_state, log_fade_factor[0], softplus_increment[0])
    backward_pass = local_sweep(jnp.flip(inputs, 0), jnp.flip(entry_state, 0), jnp.flip(readout_state, 0), jnp.flip(log_fade_factor[1], -1), jnp.flip(softplus_increment[1], -1))
    return (onward_pass, backward_pass)

def gated_norm(mixed_sum, result_switch_mapped, cluster_scaling_factor):
    gated = mixed_sum * jax.nn.silu(result_switch_mapped.astype(jnp.float32))
    grouped = gated.reshape(gated.shape[0], -1, INNER // GROUPS)
    normalized = grouped * lax.rsqrt(lax.optimization_barrier(jnp.mean(grouped * grouped, axis=-1, keepdims=True)) + EPSILON)
    return (normalized.reshape(gated.shape) * cluster_scaling_factor).astype(jnp.bfloat16)

def rms_scale(stream, gain):
    values = stream.astype(jnp.float32)
    return (values * lax.rsqrt(lax.optimization_barrier(jnp.mean(values * values, axis=-1, keepdims=True)) + EPSILON) * gain).astype(jnp.bfloat16)

def reference(skip_stream_entry, result_switch_mapped, channel_feed_mapped, write_coefficient_mapped, emission_coefficient_mapped, channel_feed_taps, write_coefficient_taps, emission_coefficient_taps, raw_increments, channel_log_fade_speed, extra_log_fade, cluster_scaling_factor, blend_result_matrix, routing_scaling_factor, specialist_switch_matrix, specialist_widen_matrix, specialist_contract_matrix, picked_specialists, router_affinities):
    rim_width = CONV_W // 2
    filter_border_width = ((rim_width, rim_width), (0, 0))
    onward_pass, backward_pass = blend_parts_list(jnp.pad(channel_feed_mapped, filter_border_width), jnp.pad(write_coefficient_mapped, filter_border_width), jnp.pad(emission_coefficient_mapped, filter_border_width), channel_feed_taps, write_coefficient_taps, emission_coefficient_taps, raw_increments, channel_log_fade_speed, extra_log_fade, SERIES_ITEMS)
    zero_carry = jnp.zeros_like(onward_pass[1][1])
    mixed_sum = finish_sweep(onward_pass[0], zero_carry) + jnp.flip(finish_sweep(backward_pass[0], zero_carry), 0)
    mixed_rows = gated_norm(mixed_sum, result_switch_mapped, cluster_scaling_factor)
    slice_width = INNER // N_TP

    def add_slice(summed, slice_index):
        columns = lax.dynamic_slice_in_dim(mixed_rows, slice_index * slice_width, slice_width, 1)
        weights = lax.dynamic_slice_in_dim(blend_result_matrix, slice_index * slice_width, slice_width, 0)
        partial_sum = jnp.dot(columns, weights, preferred_element_type=jnp.float32).astype(jnp.bfloat16)
        partial_sum = lax.optimization_barrier(partial_sum)
        return (summed + partial_sum.astype(jnp.float32), slice_index)
    projected = lax.scan(add_slice, jnp.zeros((SERIES_ITEMS, WIDTH), jnp.float32), jnp.arange(N_TP, dtype=jnp.int32))[0]
    after_mixer = (skip_stream_entry.astype(jnp.float32) + projected).astype(jnp.bfloat16)
    normed = rms_scale(after_mixer, routing_scaling_factor)
    row_count = SERIES_ITEMS * TOP
    flat_routes = picked_specialists.reshape(row_count)
    owner = jnp.arange(row_count, dtype=jnp.int32) // TOP
    limit = N_SP * N_TP * CAPACITY
    ff_slice = EXPERT_FF // N_TP

    def one_expert(outputs, expert):
        chosen = flat_routes == expert
        chosen_rank = jnp.cumsum(chosen.astype(jnp.int32)) - 1
        target = jnp.where(chosen, chosen_rank, limit)
        member = jnp.zeros((limit,), jnp.int32).at[target].set(jnp.arange(row_count, dtype=jnp.int32), mode='drop')
        filled = jnp.zeros((limit,), jnp.int32).at[target].set(1, mode='drop')
        picked = normed[owner[member]]
        gate_part = jnp.dot(picked, specialist_switch_matrix[expert], preferred_element_type=jnp.float32)
        up_part = jnp.dot(picked, specialist_widen_matrix[expert], preferred_element_type=jnp.float32)
        hidden = (jax.nn.silu(gate_part) * up_part).astype(jnp.bfloat16)
        pieces = jnp.einsum('rsf,sfd->rsd', hidden.reshape(limit, N_TP, ff_slice).astype(jnp.float32), specialist_contract_matrix[expert].reshape(N_TP, ff_slice, WIDTH).astype(jnp.float32))
        pieces = lax.optimization_barrier(pieces.astype(jnp.bfloat16))
        expert_out = lax.optimization_barrier(jnp.sum(pieces.astype(jnp.float32), axis=1)).astype(jnp.bfloat16)
        destination = jnp.where(filled > 0, member, row_count)
        return (outputs.at[destination].set(expert_out, mode='drop'), expert)
    assigned = lax.scan(one_expert, jnp.zeros((row_count, WIDTH), jnp.bfloat16), jnp.arange(EXPERTS, dtype=jnp.int32))[0]
    weights = router_affinities / lax.optimization_barrier(jnp.sum(router_affinities, axis=-1, keepdims=True))
    mixture = lax.optimization_barrier(jnp.sum(weights[..., None] * assigned.reshape(SERIES_ITEMS, TOP, WIDTH).astype(jnp.float32), axis=1))
    return (after_mixer.astype(jnp.float32) + mixture).astype(jnp.bfloat16)
```

```python
import functools

import jax
import jax.numpy as jnp
from jax import lax
from jax.experimental import pallas as pl
from jax.experimental.pallas import tpu as pltpu
from jax.sharding import PartitionSpec as P

WIDTH = 2048
HEAD_DIM = 64
GROUPS = 16
STATE = 128
CONV_W = 5
BLOCK = 128
TOP = 2
INNER = 4096


EPSILON = 1e-06
HIGHEST_MODE = lax.Precision.HIGHEST


MESH_IDS = pl.DeviceIdType.MESH
RIM = 8
EDGE = 16


def spread_heads(columns, per_group):
    rows = columns.shape[0]
    lane = lax.broadcasted_iota(jnp.int32, (rows, per_group * HEAD_DIM), 1) // HEAD_DIM
    out = jnp.broadcast_to(columns[:, 0:1], lane.shape)
    for head in range(1, per_group):
        out = jnp.where(lane == head, jnp.broadcast_to(columns[:, head : head + 1], lane.shape), out)
    return out


def silu(value):
    return value * jax.nn.sigmoid(value)


def conv_block(scratch, taps, block, lanes):
    rim = taps.shape[0] // 2
    total = None
    for offset in range(taps.shape[0]):
        start = RIM - rim + offset + block * BLOCK
        term = taps[offset : offset + 1, lanes].astype(jnp.float32) * scratch[start : start + BLOCK, lanes]
        total = term if total is None else total + term
    return silu(total)


def flip(index, mask, count):
    out, bit = index, 1
    while bit < count:
        out = out + ((mask // bit) % 2) * (1 - 2 * ((index // bit) % 2)) * bit
        bit = 2 * bit
    return out


def remote(source, target, send_sem, recv_sem, where):
    return pltpu.make_async_remote_copy(
        src_ref=source, dst_ref=target, send_sem=send_sem, recv_sem=recv_sem,
        device_id=where, device_id_type=MESH_IDS,
    )


def greet(places):
    barrier = pltpu.get_barrier_semaphore()
    for place in places:
        pl.semaphore_signal(barrier, inc=1, device_id=place, device_id_type=MESH_IDS)
    pl.semaphore_wait(barrier, len(places))


def write_route(picks_ref, affinity_ref, route_scr, experts_here, share):
    owned = picks_ref.shape[0]
    peers, core = lax.axis_size("sp"), lax.axis_index("tp") % 2
    picks, affinity = picks_ref[...], affinity_ref[...]
    lane = lax.broadcasted_iota(jnp.int32, (owned, 128), 1)
    marks = [jnp.where(picks[:, k : k + 1] == lane, 1.0, 0.0) for k in range(TOP)]
    earlier = jnp.where(
        lax.broadcasted_iota(jnp.int32, (owned, owned), 0)
        > lax.broadcasted_iota(jnp.int32, (owned, owned), 1),
        1.0,
        0.0,
    ).astype(jnp.bfloat16)
    ahead = jnp.dot(
        earlier, (marks[0] + marks[1]).astype(jnp.bfloat16), preferred_element_type=jnp.float32
    )
    base = (lane % experts_here) * (peers * share) + (lane // experts_here) * share
    base = (base + core * (share // 2)).astype(jnp.float32) + ahead
    places = [jnp.sum(mark * base, axis=1, keepdims=True) for mark in marks]
    whole = affinity[:, 0:1] + affinity[:, 1:2]
    lines = jnp.where(
        lane == 0,
        places[0],
        jnp.where(
            lane == 1,
            places[1],
            jnp.where(
                lane == 2,
                affinity[:, 0:1] / whole,
                jnp.where(lane == 3, affinity[:, 1:2] / whole, 0.0),
            ),
        ),
    )
    blank = jnp.zeros_like(lines)
    rest = [] if 2 * owned == 128 else [jnp.zeros((128 - 2 * owned, 128), jnp.float32)]
    both = jnp.concatenate(
        [jnp.where(core == 0, lines, blank), jnp.where(core == 0, blank, lines)] + rest, axis=0
    )
    route_scr[...] = jnp.transpose(both)[0:8, :]


def mixer_part(
    x_ref, b_ref, c_ref, x_taps, b_taps, c_taps, inc_ref, speed_ref, extra_ref, picks_ref,
    affinity_ref, gain_ref, norm_gain_ref, gate_ref, skip_ref, weight_ref, loads, after_ref,
    normed_ref, routes, experts_here, share,
    x_pad, b_pad, c_pad, x_low, b_low, c_low, x_high, b_high, c_high, fade_scr, x_kept, b_kept,
    c_kept, cum_scr, col_scr, entry_scr, state_ref, target, y_ref, reach_ref, carry_scr, route_scr,
    full_scr, mine_scr, give, take, ship, land,
    edge_send, edge_recv, state_send, state_recv, route_send, route_recv,
    give_send, take_recv, ship_send, land_recv,
):
    count, inner_here = x_ref.shape
    groups = b_ref.shape[1] // STATE
    width = inner_here // groups
    per_group = width // HEAD_DIM
    rows = 2 * per_group
    blocks = count // BLOCK
    rim = x_taps.shape[0] // 2
    here, peers = lax.axis_index("sp"), lax.axis_size("sp")
    seat, seats = lax.axis_index("tp"), lax.axis_size("tp")
    levels = seats // 2
    core, level = seat % 2, seat // 2
    owned, features = skip_ref.shape
    partner = {"tp": seat + 1 - 2 * core}

    edges = []
    for index, (source, low, high) in enumerate(
        ((x_ref, x_low, x_high), (b_ref, b_low, b_high), (c_ref, c_low, c_high))
    ):
        onward = remote(
            source.at[pl.ds(count - EDGE, EDGE)], low, edge_send.at[0, index],
            edge_recv.at[0, index], {"sp": lax.rem(here + 1, peers)},
        )
        back = remote(
            source.at[pl.ds(0, EDGE)], high, edge_send.at[1, index],
            edge_recv.at[1, index], {"sp": lax.rem(here + peers - 1, peers)},
        )
        edges.append((onward, back))

    @pl.when(here < peers - 1)
    def _():
        for onward, _ in edges:
            onward.start()

    @pl.when(here > 0)
    def _():
        for _, back in edges:
            back.start()

    write_route(picks_ref, affinity_ref, route_scr, experts_here, share)
    route_copies = [
        remote(
            route_scr, routes.at[seat], route_send.at[away - 1], route_recv.at[away - 1],
            {"tp": lax.rem(seat + away, seats)},
        )
        for away in range(1, seats)
    ]
    for copy in route_copies:
        copy.start()
    routes[seat] = route_scr[...]
    target[here] = jnp.zeros(target.shape[1:], target.dtype)

    heads = inc_ref.shape[1]
    square_at = [lax.broadcasted_iota(jnp.int32, (heads, heads), axis) for axis in range(2)]
    for first in range(2):
        raw = inc_ref[first].astype(jnp.float32)
        step = jnp.maximum(raw, 0.0) + jnp.log1p(jnp.exp(-jnp.abs(raw)))
        line = jnp.broadcast_to(speed_ref[first : first + 1, :], (heads, heads))
        speed = jnp.sum(
            jnp.where(square_at[0] == square_at[1], jnp.exp(line), 0.0), axis=1, keepdims=True
        )
        fade = -step * speed + extra_ref[first]
        for group in range(groups):
            mine = slice(group * per_group, (group + 1) * per_group)
            spot = first * per_group
            fade_scr[group, spot : spot + per_group, :] = fade[mine, :]
            fade_scr[group, rows + spot : rows + spot + per_group, :] = step[mine, :]
    for pad, source in ((x_pad, x_ref), (b_pad, b_ref), (c_pad, c_ref)):
        pad[RIM : RIM + count, :] = source[...].astype(jnp.float32)

    @pl.when(here > 0)
    def _():
        for onward, _ in edges:
            onward.wait_recv()
        for pad, low in ((x_pad, x_low), (b_pad, b_low), (c_pad, c_low)):
            pad[RIM - rim : RIM, :] = low[...].astype(jnp.float32)[EDGE - rim : EDGE, :]

    @pl.when(here == 0)
    def _():
        for pad in (x_pad, b_pad, c_pad):
            pad[RIM - rim : RIM, :] = jnp.zeros((rim, pad.shape[1]), jnp.float32)

    @pl.when(here < peers - 1)
    def _():
        for _, back in edges:
            back.wait_recv()
        for pad, high in ((x_pad, x_high), (b_pad, b_high), (c_pad, c_high)):
            pad[RIM + count : RIM + count + rim, :] = high[...].astype(jnp.float32)[0:rim, :]

    @pl.when(here == peers - 1)
    def _():
        for pad in (x_pad, b_pad, c_pad):
            pad[RIM + count : RIM + count + rim, :] = jnp.zeros((rim, pad.shape[1]), jnp.float32)

    i_at = lax.broadcasted_iota(jnp.int32, (BLOCK, BLOCK), 0)
    j_at = lax.broadcasted_iota(jnp.int32, (BLOCK, BLOCK), 1)
    up_to = (i_at <= j_at).astype(jnp.float32)
    from_on = (i_at >= j_at).astype(jnp.float32)
    row_at = lax.broadcasted_iota(jnp.int32, (rows, BLOCK), 0)
    col_at = lax.broadcasted_iota(jnp.int32, (1, rows), 1)
    half_lane = lax.broadcasted_iota(jnp.int32, (BLOCK, 2 * HEAD_DIM), 1) < HEAD_DIM

    def state_copy(group, away):
        peer = lax.rem(here + away, peers)
        return remote(
            state_ref.at[jnp.where(peer > here, 0, 1), group], target.at[here, group],
            state_send.at[group, away - 1], state_recv.at[group, away - 1], {"sp": peer},
        )

    all_totals = []
    for group in range(groups):
        lanes_x = slice(group * width, (group + 1) * width)
        lanes_s = slice(group * STATE, (group + 1) * STATE)
        totals, parts = [], []
        for block in range(blocks):
            at = slice(block * BLOCK, (block + 1) * BLOCK)
            fade = fade_scr[group, 0:rows, at]
            step = fade_scr[group, rows : 2 * rows, at]
            onward = jnp.dot(fade, up_to, precision=HIGHEST_MODE, preferred_element_type=jnp.float32)
            back = jnp.dot(fade, from_on, precision=HIGHEST_MODE, preferred_element_type=jnp.float32)
            cum = jnp.where(row_at < per_group, onward, back)
            stacked = jnp.concatenate(
                [cum, step, jnp.zeros((BLOCK - 2 * rows, BLOCK), jnp.float32)], axis=0
            )
            turned = jnp.transpose(stacked)
            cum_col, step_col = turned[:, 0:rows], turned[:, rows : 2 * rows]
            total = jnp.where(col_at < per_group, cum_col[BLOCK - 1 : BLOCK, :], cum_col[0:1, :])
            to_end = jnp.exp(total - cum_col) * step_col
            cum_scr[group, block] = cum
            col_scr[group, block] = cum_col
            x = conv_block(x_pad, x_taps, block, lanes_x)
            b = conv_block(b_pad, b_taps, block, lanes_s)
            x_kept[at, lanes_x] = x
            b_turned = jnp.transpose(b).astype(jnp.bfloat16)
            b_kept[group, block] = b_turned
            weighted = jnp.concatenate(
                [
                    x * spread_heads(to_end[:, 0:per_group], per_group),
                    x * spread_heads(to_end[:, per_group:rows], per_group),
                ],
                axis=1,
            ).astype(jnp.bfloat16)
            parts.append(jnp.dot(b_turned, weighted, preferred_element_type=jnp.float32))
            totals.append(total)
        for first, order in ((0, range(blocks)), (1, range(blocks - 1, -1, -1))):
            lanes = slice(first * width, (first + 1) * width)
            held = jnp.zeros((STATE, width), jnp.float32)
            for block in order:
                entry_scr[group, block, :, lanes] = held.astype(jnp.bfloat16)
                factor = spread_heads(
                    jnp.exp(totals[block][:, first * per_group : (first + 1) * per_group]), per_group
                )
                held = held * factor + parts[block][:, lanes]
            state_ref[first, group, 0:STATE, :] = held.astype(jnp.bfloat16)
            whole = totals[0]
            for block in range(1, blocks):
                whole = whole + totals[block]
            whole = spread_heads(
                jnp.exp(whole[:, first * per_group : (first + 1) * per_group]), per_group
            )
            state_ref[first, group, STATE:, :] = jnp.broadcast_to(
                whole, (state_ref.shape[2] - STATE, width)
            ).astype(jnp.bfloat16)
        for away in range(1, peers):
            state_copy(group, away).start()
        all_totals.append(totals)

    for group in range(groups):
        lanes_x = slice(group * width, (group + 1) * width)
        lanes_s = slice(group * STATE, (group + 1) * STATE)
        totals = all_totals[group]
        for block in range(blocks):
            at = slice(block * BLOCK, (block + 1) * BLOCK)
            step = fade_scr[group, rows : 2 * rows, at]
            cum, cum_col = cum_scr[group, block], col_scr[group, block]
            x = x_kept[at, lanes_x]
            c = conv_block(c_pad, c_taps, block, lanes_s).astype(jnp.bfloat16)
            c_kept[at, lanes_s] = c
            inner = jnp.dot(c, b_kept[group, block], preferred_element_type=jnp.float32)
            mixing = []
            for head in range(per_group):
                other = per_group + head
                gap = jnp.where(
                    i_at >= j_at,
                    cum_col[:, head : head + 1] - cum[head : head + 1, :],
                    cum_col[:, other : other + 1] - cum[other : other + 1, :],
                )
                own, opposite = step[head : head + 1, :], step[other : other + 1, :]
                amount = jnp.where(
                    i_at > j_at, own, jnp.where(i_at < j_at, opposite, own + opposite)
                )
                mixing.append((jnp.exp(gap) * amount * inner).astype(jnp.bfloat16))
            pieces = []
            for pair in range(per_group // 2):
                x_pair = x[:, pair * 2 * HEAD_DIM : (pair + 1) * 2 * HEAD_DIM]
                both = jnp.concatenate(
                    [jnp.where(half_lane, x_pair, 0.0), jnp.where(half_lane, 0.0, x_pair)], axis=0
                ).astype(jnp.bfloat16)
                left = jnp.concatenate([mixing[2 * pair], mixing[2 * pair + 1]], axis=1)
                pieces.append(jnp.dot(left, both, preferred_element_type=jnp.float32))
            readout = jnp.dot(c, entry_scr[group, block], preferred_element_type=jnp.float32)
            fade_in = jnp.exp(cum_col)
            y_ref[at, lanes_x] = (
                jnp.concatenate(pieces, axis=1)
                + readout[:, :width] * spread_heads(fade_in[:, 0:per_group], per_group)
                + readout[:, width:] * spread_heads(fade_in[:, per_group:rows], per_group)
            )
            offset = jnp.zeros((1, rows), jnp.float32)
            for earlier in range(blocks):
                if earlier < block:
                    offset = offset + jnp.where(col_at < per_group, totals[earlier], 0.0)
                if earlier > block:
                    offset = offset + jnp.where(col_at < per_group, 0.0, totals[earlier])
            reach_ref[group, at, :] = jnp.exp(cum_col + offset)

    def at_level(mask):
        return {"tp": 2 * flip(level, mask, levels) + core}

    def hand(mask):
        return remote(give.at[mask], take.at[mask], give_send.at[mask], take_recv.at[mask], partner)

    def post(mask):
        return remote(
            ship.at[mask], land.at[mask], ship_send.at[mask], land_recv.at[mask], at_level(mask)
        )

    for load in loads:
        load.wait()
    for group in range(groups):
        for away in range(1, peers):
            state_copy(group, away).wait_recv()
        for first in range(2):
            held = jnp.zeros((STATE, width), jnp.float32)
            order = range(peers) if first == 0 else range(peers - 1, -1, -1)
            for peer in order:
                fresh = target[peer, group, 0:STATE, :].astype(jnp.float32)
                factor = target[peer, group, STATE : STATE + 1, :].astype(jnp.float32)
                reached = peer < here if first == 0 else peer > here
                held = jnp.where(reached, held * factor + fresh, held)
            carry_scr[group, :, first * width : (first + 1) * width] = held.astype(jnp.bfloat16)

    def pass_on(mask):
        hand(mask).wait_recv()
        ship[mask] = (mine_scr[mask] + take[mask].astype(jnp.float32)).astype(jnp.bfloat16)
        post(mask).start()

    def one_block(turn, _):
        mask = levels - 1 - turn
        at = pl.ds(pl.multiple_of(flip(level, mask, levels) * (2 * owned), 2 * owned), 2 * owned)
        mixed = []
        for group in range(groups):
            lanes = slice(group * width, (group + 1) * width)
            c = c_kept[at, group * STATE : (group + 1) * STATE]
            readout = jnp.dot(c, carry_scr[group], preferred_element_type=jnp.float32)
            reach = reach_ref[group, at, :]
            y = (
                y_ref[at, lanes]
                + readout[:, :width] * spread_heads(reach[:, 0:per_group], per_group)
                + readout[:, width:] * spread_heads(reach[:, per_group:rows], per_group)
            )
            gated = y * silu(gate_ref[at, lanes].astype(jnp.float32))
            square = jnp.mean(gated * gated, axis=-1, keepdims=True)
            mixed.append(
                (gated * lax.rsqrt(square + EPSILON) * gain_ref[:, lanes]).astype(jnp.bfloat16)
            )
        rows_mixed = mixed[0] if groups == 1 else jnp.concatenate(mixed, axis=1)
        tile = min(512, features)
        for start in range(0, features, tile):
            full_scr[:, start : start + tile] = jnp.dot(
                rows_mixed, weight_ref[:, start : start + tile], preferred_element_type=jnp.float32
            )
        own = pl.multiple_of(core * owned, owned)
        other = pl.multiple_of((1 - core) * owned, owned)
        give[mask] = full_scr[pl.ds(other, owned), :].astype(jnp.bfloat16)
        hand(mask).start()
        mine_scr[mask] = full_scr[pl.ds(own, owned), :]

        @pl.when(turn > 0)
        def _():
            pass_on(mask + 1)

        return 0

    lax.fori_loop(0, levels, one_block, 0)
    hand(0).wait_recv()
    total = mine_scr[0] + take[0].astype(jnp.float32)
    for mask in range(1, levels):
        post(mask).wait_recv()
        total = total + land[mask].astype(jnp.float32)
    after = (skip_ref[...].astype(jnp.float32) + total).astype(jnp.bfloat16)
    after_ref[...] = after
    values = after.astype(jnp.float32)
    scale = lax.rsqrt(jnp.mean(values * values, axis=-1, keepdims=True) + EPSILON)
    normed_ref[...] = (values * scale * norm_gain_ref[...]).astype(jnp.bfloat16)
    for copy in route_copies:
        copy.wait_recv()

    def settle():
        for mask in range(levels):
            hand(mask).wait_send()
            if mask:
                post(mask).wait_send()
        for copy in route_copies:
            copy.wait_send()
        for group in range(groups):
            for away in range(1, peers):
                state_copy(group, away).wait_send()

        @pl.when(here < peers - 1)
        def _():
            for onward, _ in edges:
                onward.wait_send()

        @pl.when(here > 0)
        def _():
            for _, back in edges:
                back.wait_send()

    return settle


AHEAD = 2


def experts_part(
    normed_ref, after_ref, routes_ref, out_ref, loads, settle,
    rows_scr, stage, own_in, other_in, other_out, other_got, kept, hidden, returned,
    full_scr, mine_scr, give, take, ship, land, gate_w, up_w, down_w,
    row_send, row_recv, pair_send, pair_recv, out_send, out_recv, side_send, side_recv,
    sum_send, sum_recv, back_send, back_recv, give_send, take_recv, ship_send, land_recv,
):
    here, peers = lax.axis_index("sp"), lax.axis_size("sp")
    seat = lax.axis_index("tp")
    levels = lax.axis_size("tp") // 2
    core, level = seat % 2, seat // 2
    owned, features = normed_ref.shape
    share = stage.shape[2]
    slots = peers * share
    tokens = 2 * owned
    partner = {"tp": seat + 1 - 2 * core}
    away_order = list(range(peers - 1, 0, -1))

    def floor_of(mask):
        return flip(level, mask, levels)

    def at_level(mask):
        return {"tp": 2 * floor_of(mask) + core}

    def column(away):
        return flip(here, away, peers)

    def row_copy(mask):
        return remote(
            normed_ref, rows_scr.at[level, core], row_send.at[mask], row_recv.at[mask],
            at_level(mask),
        )

    def pair_copy(mask):
        spot = rows_scr.at[floor_of(mask), core]
        source = normed_ref if isinstance(mask, int) and mask == 0 else spot
        return remote(source, spot, pair_send.at[mask], pair_recv.at[mask], partner)

    def out_copy(mask, away):
        floor = floor_of(mask)
        return remote(
            stage.at[floor, column(away)], own_in.at[floor, here],
            out_send.at[mask, away], out_recv.at[mask, away], {"sp": column(away)},
        )

    def side_copy(mask, away):
        return remote(
            own_in.at[floor_of(mask), column(away)], other_in.at[mask % 2, column(away)],
            side_send.at[mask, away], side_recv.at[mask, away], partner,
        )

    def sum_copy(mask):
        return remote(
            other_out.at[mask % 2], other_got.at[mask % 2], sum_send.at[mask], sum_recv.at[mask],
            partner,
        )

    def back_copy(mask, away):
        floor = floor_of(mask)
        return remote(
            stage.at[floor, column(away)], returned.at[floor, here],
            back_send.at[mask, away], back_recv.at[mask, away], {"sp": column(away)},
        )

    def hand(mask):
        return remote(give.at[mask], take.at[mask], give_send.at[mask], take_recv.at[mask], partner)

    def post(mask):
        return remote(
            ship.at[mask], land.at[mask], ship_send.at[mask], land_recv.at[mask], at_level(mask)
        )

    rows_scr[level, core] = normed_ref[...]
    for mask in range(1, levels):
        row_copy(mask).start()

    def routes_of(mask):
        floor = floor_of(mask)
        return routes_ref[2 * floor] + routes_ref[2 * floor + 1]

    def dispatch(mask):
        floor = floor_of(mask)
        pair_copy(mask).start()
        tile = routes_of(mask)
        code = (
            lax.broadcasted_iota(jnp.int32, (slots, tokens), 0) + core * slots
        ).astype(jnp.float32)
        chosen = (tile[0:1, 0:tokens] == code) | (tile[1:2, 0:tokens] == code)
        chosen = jnp.where(chosen, 1.0, 0.0).astype(jnp.bfloat16)
        pair_copy(mask).wait_recv()
        width = min(512, features)
        for start in range(0, features, width):
            lanes = slice(start, start + width)
            rows = rows_scr[floor, :, :, lanes].reshape(tokens, width)
            picked = jnp.dot(chosen, rows, preferred_element_type=jnp.float32)
            stage[floor, :, :, lanes] = picked.astype(jnp.bfloat16).reshape(peers, share, width)
        own_in[floor, here] = stage[floor, here]
        for away in away_order:
            out_copy(mask, away).start()

    def arrive_and_dispatch(mask):
        row_copy(mask).wait_recv()
        dispatch(mask)

    dispatch(0)
    for mask in range(1, min(AHEAD, levels)):
        arrive_and_dispatch(mask)
    for load in loads:
        load.wait()

    def expert(index, source, store):
        hid = gate_w.shape[2]
        width = min(256, hid)

        def up_tile(n, _):
            lanes = pl.ds(pl.multiple_of(n * width, width), width)
            x = source[...].reshape(slots, features)
            gate = jnp.dot(x, gate_w[index, :, lanes], preferred_element_type=jnp.float32)
            up = jnp.dot(x, up_w[index, :, lanes], preferred_element_type=jnp.float32)
            hidden[:, lanes] = (silu(gate) * up).astype(jnp.bfloat16)
            return 0

        lax.fori_loop(0, hid // width, up_tile, 0)
        wide = min(512, features)

        def down_tile(n, _):
            lanes = pl.ds(pl.multiple_of(n * wide, wide), wide)
            store(
                lanes,
                jnp.dot(hidden[...], down_w[index, :, lanes], preferred_element_type=jnp.float32),
            )
            return 0

        lax.fori_loop(0, features // wide, down_tile, 0)

    def one_floor(mask, _):
        floor = floor_of(mask)
        side_copy(mask, 0).start()
        for away in away_order:
            out_copy(mask, away).wait_recv()
            side_copy(mask, away).start()
        if AHEAD < levels:

            @pl.when(mask + AHEAD < levels)
            def _():
                arrive_and_dispatch(mask + AHEAD)

        for away in range(peers):
            side_copy(mask, away).wait_recv()

        @pl.when(mask >= 2)
        def _():
            sum_copy(mask - 2).wait_send()

        def give_out(lanes, value):
            other_out[mask % 2, :, lanes] = value.astype(jnp.bfloat16)

        def keep(lanes, value):
            kept[:, lanes] = value

        expert(1 - core, other_in.at[mask % 2], give_out)
        sum_copy(mask).start()
        expert(core, own_in.at[floor], keep)
        for away in away_order:
            out_copy(mask, away).wait_send()
        sum_copy(mask).wait_recv()
        both = (kept[...] + other_got[mask % 2].astype(jnp.float32)).astype(jnp.bfloat16)
        stage[floor] = both.reshape(peers, share, features)
        returned[floor, here] = stage[floor, here]

        @pl.when(mask > 0)
        def _():
            for away in away_order:
                back_copy(mask, away).start()

        return 0

    lax.fori_loop(0, levels, one_floor, 0)
    for away in away_order:
        back_copy(0, away).start()

    def pass_on(mask):
        hand(mask).wait_recv()
        ship[mask] = (mine_scr[mask] + take[mask].astype(jnp.float32)).astype(jnp.bfloat16)
        post(mask).start()

    def combine(turn, _):
        mask = (turn + 1) % levels
        tile = routes_of(mask)
        size = tile.shape[1]
        turned = jnp.transpose(
            jnp.concatenate([tile, jnp.zeros((size - tile.shape[0], size), jnp.float32)], axis=0)
        )[0:tokens, :]
        code = (
            lax.broadcasted_iota(jnp.int32, (tokens, slots), 1) + core * slots
        ).astype(jnp.float32)
        weight = jnp.where(turned[:, 0:1] == code, turned[:, 2:3], 0.0) + jnp.where(
            turned[:, 1:2] == code, turned[:, 3:4], 0.0
        )
        high = weight.astype(jnp.bfloat16)
        low = (weight - high.astype(jnp.float32)).astype(jnp.bfloat16)
        for away in away_order:
            back_copy(mask, away).wait_recv()
        width = min(512, features)
        for start in range(0, features, width):
            lanes = slice(start, start + width)
            got = returned[floor_of(mask), :, :, lanes].reshape(slots, width)
            full_scr[:, lanes] = jnp.dot(
                high, got, preferred_element_type=jnp.float32
            ) + jnp.dot(low, got, preferred_element_type=jnp.float32)
        own = pl.multiple_of(core * owned, owned)
        other = pl.multiple_of((1 - core) * owned, owned)
        give[mask] = full_scr[pl.ds(other, owned), :].astype(jnp.bfloat16)
        hand(mask).start()
        mine_scr[mask] = full_scr[pl.ds(own, owned), :]

        @pl.when(turn > 0)
        def _():
            pass_on(turn)

        return 0

    settle()
    lax.fori_loop(0, levels, combine, 0)
    hand(0).wait_recv()
    total = mine_scr[0] + take[0].astype(jnp.float32)
    for mask in range(1, levels):
        post(mask).wait_recv()
        total = total + land[mask].astype(jnp.float32)
    out_ref[...] = (after_ref[...].astype(jnp.float32) + total).astype(jnp.bfloat16)

    for mask in range(levels):
        pair_copy(mask).wait_send()
        hand(mask).wait_send()
        if mask:
            row_copy(mask).wait_send()
            post(mask).wait_send()
        if mask + 2 >= levels:
            sum_copy(mask).wait_send()
        for away in range(peers):
            side_copy(mask, away).wait_send()
            if away:
                back_copy(mask, away).wait_send()


def layer_kernel(experts_here, share, counts, *refs):
    refs = list(refs)

    def take(number):
        out = refs[:number]
        del refs[:number]
        return out

    near = take(counts[0])
    far = take(counts[1])
    (out_ref,) = take(1)
    loaded = take(counts[1])
    after_ref, normed_ref, routes = take(3)
    mixer_own = take(counts[2])
    shared = take(6)
    mixer_flags = take(10)
    experts_own = take(9)
    experts_flags = take(16)
    (load_sem,) = take(1)
    loads = [
        pltpu.make_async_copy(source, target, load_sem.at[index])
        for index, (source, target) in enumerate(zip(far, loaded))
    ]
    for load in loads:
        load.start()
    here, peers = lax.axis_index("sp"), lax.axis_size("sp")
    seat, seats = lax.axis_index("tp"), lax.axis_size("tp")
    greet(
        [{"sp": lax.rem(here + away, peers)} for away in range(1, peers)]
        + [{"tp": lax.rem(seat + away, seats)} for away in range(1, seats)]
    )
    settle = mixer_part(
        *near, *loaded[0:3], loads[0:3], after_ref, normed_ref, routes, experts_here, share,
        *mixer_own, *shared, *mixer_flags,
    )
    experts_part(
        normed_ref, after_ref, routes, out_ref, loads[3:], settle,
        *experts_own, *shared, *loaded[3:], *experts_flags,
    )


def per_device(
    skip_stream_entry,
    result_switch_mapped,
    channel_feed_mapped,
    write_coefficient_mapped,
    emission_coefficient_mapped,
    channel_feed_taps,
    write_coefficient_taps,
    emission_coefficient_taps,
    raw_increments,
    channel_log_fade_speed,
    extra_log_fade,
    cluster_scaling_factor,
    blend_result_matrix,
    routing_scaling_factor,
    specialist_switch_matrix,
    specialist_widen_matrix,
    specialist_contract_matrix,
    picked_specialists,
    router_affinities,
):
    count, inner_here = channel_feed_mapped.shape
    owned, features = skip_stream_entry.shape
    experts_here, _, units = specialist_switch_matrix.shape
    peers, seats = lax.axis_size("sp"), lax.axis_size("tp")
    levels = seats // 2
    groups = write_coefficient_mapped.shape[1] // STATE
    width = inner_here // groups
    rows = 2 * (width // HEAD_DIM)
    blocks = count // BLOCK
    depth = STATE + 16
    capacity = max(2, 3 * TOP * owned // (2 * experts_here * peers))
    share = 2 * (-(-capacity // 8) * 8)
    slots = peers * share
    vmem, anywhere = pl.BlockSpec(memory_space=pltpu.VMEM), pl.BlockSpec(memory_space=pl.ANY)

    def half(*shape):
        return pltpu.VMEM(shape, jnp.bfloat16)

    def full(*shape):
        return pltpu.VMEM(shape, jnp.float32)

    def flags(*shape):
        return pltpu.SemaphoreType.DMA(shape)

    near = [
        channel_feed_mapped, write_coefficient_mapped, emission_coefficient_mapped,
        channel_feed_taps, write_coefficient_taps, emission_coefficient_taps, raw_increments,
        channel_log_fade_speed, extra_log_fade, picked_specialists, router_affinities,
        cluster_scaling_factor.reshape(1, -1), routing_scaling_factor.reshape(1, -1),
    ]
    far = [
        result_switch_mapped, skip_stream_entry, blend_result_matrix,
        specialist_switch_matrix, specialist_widen_matrix, specialist_contract_matrix,
    ]
    lines = groups * STATE
    mixer_own = [
        full(count + 2 * RIM, inner_here), full(count + 2 * RIM, lines), full(count + 2 * RIM, lines),
        half(EDGE, inner_here), half(EDGE, lines), half(EDGE, lines),
        half(EDGE, inner_here), half(EDGE, lines), half(EDGE, lines),
        full(groups, 2 * rows, count), full(count, inner_here), half(groups, blocks, STATE, BLOCK),
        half(count, lines), full(groups, blocks, rows, BLOCK), full(groups, blocks, BLOCK, rows),
        half(groups, blocks, STATE, 2 * width), half(2, groups, depth, width),
        half(peers, groups, depth, width), full(count, inner_here), full(groups, count, rows),
        half(groups, STATE, 2 * width), full(8, 128),
    ]
    slab = (levels, owned, features)
    shared = [full(2 * owned, features), full(*slab)] + [half(*slab)] * 4
    mixer_flags = [
        flags(2, 3), flags(2, 3), flags(groups, peers - 1), flags(groups, peers - 1),
        flags(seats - 1), flags(seats - 1), flags(levels), flags(levels), flags(levels), flags(levels),
    ]
    experts_own = [
        half(levels, 2, owned, features),
        half(levels, peers, share, features),
        half(levels, peers, share, features),
        half(2, peers, share, features),
        half(2, slots, features),
        half(2, slots, features),
        full(slots, features),
        half(slots, units),
        half(levels, peers, share, features),
    ]
    experts_flags = [
        flags(levels), flags(levels), flags(levels), flags(levels),
        flags(levels, peers), flags(levels, peers), flags(levels, peers), flags(levels, peers),
        flags(levels), flags(levels), flags(levels, peers), flags(levels, peers),
        flags(levels), flags(levels), flags(levels), flags(levels),
    ]
    return pl.pallas_call(
        functools.partial(layer_kernel, experts_here, share, (len(near), len(far), len(mixer_own))),
        in_specs=[vmem] * len(near) + [anywhere] * len(far),
        out_specs=vmem,
        out_shape=jax.ShapeDtypeStruct((owned, features), jnp.bfloat16),
        scratch_shapes=[half(*array.shape) for array in far]
        + [half(owned, features), half(owned, features), full(seats, 8, 128)]
        + mixer_own + shared + mixer_flags + experts_own + experts_flags + [flags(len(far))],
        compiler_params=pltpu.CompilerParams(
            collective_id=0, has_side_effects=True, vmem_limit_bytes=67043328
        ),
        name="layer",
    )(*near, *far)


def solution(mesh):
    in_specs = (
        P(("sp", "tp"), None),
        P("sp", "tp"),
        P("sp", "tp"),
        P("sp", "tp"),
        P("sp", "tp"),
        P(None, "tp"),
        P(None, "tp"),
        P(None, "tp"),
        P(None, "tp", "sp"),
        P(None, "tp"),
        P(None, "tp", "sp"),
        P("tp"),
        P("tp", None),
        P(),
        P("sp", None, "tp"),
        P("sp", None, "tp"),
        P("sp", "tp", None),
        P(("sp", "tp"), None),
        P(("sp", "tp"), None),
    )
    out_specs = P(("sp", "tp"), None)
    return jax.shard_map(
        per_device, mesh=mesh, in_specs=in_specs, out_specs=out_specs, check_vma=False
    )
```

```python
import functools

import jax
import jax.numpy as jnp
from jax import lax
from jax.experimental import pallas as pl
from jax.experimental.pallas import tpu as pltpu
from jax.sharding import PartitionSpec as P

WIDTH = 2048
HEAD_DIM = 64
GROUPS = 16
STATE = 128
CONV_W = 5
BLOCK = 128
TOP = 2
INNER = 4096


EPSILON = 1e-06
HIGHEST_MODE = lax.Precision.HIGHEST


MESH_IDS = pl.DeviceIdType.MESH
RIM = 8
EDGE = 16


def spread_heads(columns, per_group):
    rows = columns.shape[0]
    lane = lax.broadcasted_iota(jnp.int32, (rows, per_group * HEAD_DIM), 1) // HEAD_DIM
    out = jnp.broadcast_to(columns[:, 0:1], lane.shape)
    for head in range(1, per_group):
        out = jnp.where(lane == head, jnp.broadcast_to(columns[:, head : head + 1], lane.shape), out)
    return out


def silu(value):
    return value * jax.nn.sigmoid(value)


def conv_block(scratch, taps, block, lanes):
    rim = taps.shape[0] // 2
    total = None
    for offset in range(taps.shape[0]):
        start = RIM - rim + offset + block * BLOCK
        term = taps[offset : offset + 1, lanes].astype(jnp.float32) * scratch[start : start + BLOCK, lanes]
        total = term if total is None else total + term
    return silu(total)


def flip(index, mask, count):
    out, bit = index, 1
    while bit < count:
        out = out + ((mask // bit) % 2) * (1 - 2 * ((index // bit) % 2)) * bit
        bit = 2 * bit
    return out


def low_bit(mask, count):
    out, bit = 0, count // 2
    while bit >= 1:
        odd = (mask // bit) % 2
        out = odd * bit + (1 - odd) * out
        bit = bit // 2
    return out


def remote(source, target, send_sem, recv_sem, where):
    return pltpu.make_async_remote_copy(
        src_ref=source, dst_ref=target, send_sem=send_sem, recv_sem=recv_sem,
        device_id=where, device_id_type=MESH_IDS,
    )


def greet(places):
    barrier = pltpu.get_barrier_semaphore()
    for place in places:
        pl.semaphore_signal(barrier, inc=1, device_id=place, device_id_type=MESH_IDS)
    pl.semaphore_wait(barrier, len(places))


def write_route(picks_ref, affinity_ref, route_scr, experts_here, share):
    owned = picks_ref.shape[1]
    peers, core = lax.axis_size("sp"), lax.axis_index("tp") % 2
    picks, affinity = picks_ref[...], affinity_ref[...]
    count = -(-experts_here * peers // 8) * 8
    expert = lax.broadcasted_iota(jnp.int32, (count, owned), 0)
    marks = [jnp.where(picks[k : k + 1, :] == expert, 1.0, 0.0) for k in range(TOP)]
    earlier = jnp.where(
        lax.broadcasted_iota(jnp.int32, (owned, owned), 0)
        < lax.broadcasted_iota(jnp.int32, (owned, owned), 1),
        1.0,
        0.0,
    ).astype(jnp.bfloat16)
    ahead = jnp.dot(
        (marks[0] + marks[1]).astype(jnp.bfloat16), earlier, preferred_element_type=jnp.float32
    )
    base = (expert % experts_here) * (peers * share) + (expert // experts_here) * share
    base = (base + core * (share // 2)).astype(jnp.float32) + ahead
    places = [jnp.sum(mark * base, axis=0, keepdims=True) for mark in marks]
    whole = affinity[0:1, :] + affinity[1:2, :]
    lines = jnp.concatenate(
        places
        + [affinity[0:1, :] / whole, affinity[1:2, :] / whole]
        + [jnp.zeros((8 - 2 * TOP, owned), jnp.float32)],
        axis=0,
    )
    blank = jnp.zeros_like(lines)
    rest = [] if 2 * owned == 128 else [jnp.zeros((8, 128 - 2 * owned), jnp.float32)]
    route_scr[...] = jnp.concatenate(
        [jnp.where(core == 0, lines, blank), jnp.where(core == 0, blank, lines)] + rest, axis=1
    )


def mixer_part(
    x_ref, b_ref, c_ref, x_taps, b_taps, c_taps, inc_ref, speed_ref, extra_ref, picks_ref,
    affinity_ref, gain_ref, norm_gain_ref, gate_ref, skip_ref, weight_ref, loads, after_ref,
    normed_ref, routes, experts_here, share,
    x_pad, b_pad, c_pad, x_low, b_low, c_low, x_high, b_high, c_high, fade_scr, x_kept, b_kept,
    c_kept, cum_scr, col_scr, entry_scr, state_ref, target, y_ref, reach_ref, carry_scr, route_scr,
    full_scr, mine_scr, give, take, ship, land,
    edge_send, edge_recv, state_send, state_recv, route_send, route_recv,
    give_send, take_recv, ship_send, land_recv,
):
    count, inner_here = x_ref.shape
    groups = b_ref.shape[1] // STATE
    width = inner_here // groups
    per_group = width // HEAD_DIM
    rows = 2 * per_group
    blocks = count // BLOCK
    rim = x_taps.shape[0] // 2
    here, peers = lax.axis_index("sp"), lax.axis_size("sp")
    seat, seats = lax.axis_index("tp"), lax.axis_size("tp")
    levels = seats // 2
    core, level = seat % 2, seat // 2
    owned, features = skip_ref.shape
    partner = {"tp": seat + 1 - 2 * core}

    edges = []
    for index, (source, low, high) in enumerate(
        ((x_ref, x_low, x_high), (b_ref, b_low, b_high), (c_ref, c_low, c_high))
    ):
        onward = remote(
            source.at[pl.ds(count - EDGE, EDGE)], low, edge_send.at[0, index],
            edge_recv.at[0, index], {"sp": lax.rem(here + 1, peers)},
        )
        back = remote(
            source.at[pl.ds(0, EDGE)], high, edge_send.at[1, index],
            edge_recv.at[1, index], {"sp": lax.rem(here + peers - 1, peers)},
        )
        edges.append((onward, back))

    @pl.when(here < peers - 1)
    def _():
        for onward, _ in edges:
            onward.start()

    @pl.when(here > 0)
    def _():
        for _, back in edges:
            back.start()

    write_route(picks_ref, affinity_ref, route_scr, experts_here, share)
    route_copies = [
        remote(
            route_scr, routes.at[seat], route_send.at[away - 1], route_recv.at[away - 1],
            {"tp": lax.rem(seat + away, seats)},
        )
        for away in range(1, seats)
    ]
    for copy in route_copies:
        copy.start()
    routes[seat] = route_scr[...]
    target[here] = jnp.zeros(target.shape[1:], target.dtype)

    heads = inc_ref.shape[1]
    square_at = [lax.broadcasted_iota(jnp.int32, (heads, heads), axis) for axis in range(2)]
    for first in range(2):
        raw = inc_ref[first].astype(jnp.float32)
        step = jnp.maximum(raw, 0.0) + jnp.log1p(jnp.exp(-jnp.abs(raw)))
        line = jnp.broadcast_to(speed_ref[first : first + 1, :], (heads, heads))
        speed = jnp.sum(
            jnp.where(square_at[0] == square_at[1], jnp.exp(line), 0.0), axis=1, keepdims=True
        )
        fade = -step * speed + extra_ref[first]
        for group in range(groups):
            mine = slice(group * per_group, (group + 1) * per_group)
            spot = first * per_group
            fade_scr[group, spot : spot + per_group, :] = fade[mine, :]
            fade_scr[group, rows + spot : rows + spot + per_group, :] = step[mine, :]
    for pad, source in ((x_pad, x_ref), (b_pad, b_ref), (c_pad, c_ref)):
        pad[RIM : RIM + count, :] = source[...].astype(jnp.float32)

    @pl.when(here > 0)
    def _():
        for onward, _ in edges:
            onward.wait_recv()
        for pad, low in ((x_pad, x_low), (b_pad, b_low), (c_pad, c_low)):
            pad[RIM - rim : RIM, :] = low[...].astype(jnp.float32)[EDGE - rim : EDGE, :]

    @pl.when(here == 0)
    def _():
        for pad in (x_pad, b_pad, c_pad):
            pad[RIM - rim : RIM, :] = jnp.zeros((rim, pad.shape[1]), jnp.float32)

    @pl.when(here < peers - 1)
    def _():
        for _, back in edges:
            back.wait_recv()
        for pad, high in ((x_pad, x_high), (b_pad, b_high), (c_pad, c_high)):
            pad[RIM + count : RIM + count + rim, :] = high[...].astype(jnp.float32)[0:rim, :]

    @pl.when(here == peers - 1)
    def _():
        for pad in (x_pad, b_pad, c_pad):
            pad[RIM + count : RIM + count + rim, :] = jnp.zeros((rim, pad.shape[1]), jnp.float32)

    i_at = lax.broadcasted_iota(jnp.int32, (BLOCK, BLOCK), 0)
    j_at = lax.broadcasted_iota(jnp.int32, (BLOCK, BLOCK), 1)
    up_to = (i_at <= j_at).astype(jnp.float32)
    from_on = (i_at >= j_at).astype(jnp.float32)
    row_at = lax.broadcasted_iota(jnp.int32, (rows, BLOCK), 0)
    col_at = lax.broadcasted_iota(jnp.int32, (1, rows), 1)
    half_lane = lax.broadcasted_iota(jnp.int32, (BLOCK, 2 * HEAD_DIM), 1) < HEAD_DIM

    def state_copy(group, away):
        peer = lax.rem(here + away, peers)
        return remote(
            state_ref.at[jnp.where(peer > here, 0, 1), group], target.at[here, group],
            state_send.at[group, away - 1], state_recv.at[group, away - 1], {"sp": peer},
        )

    all_totals = []
    for group in range(groups):
        lanes_x = slice(group * width, (group + 1) * width)
        lanes_s = slice(group * STATE, (group + 1) * STATE)
        totals, parts = [], []
        for block in range(blocks):
            at = slice(block * BLOCK, (block + 1) * BLOCK)
            fade = fade_scr[group, 0:rows, at]
            step = fade_scr[group, rows : 2 * rows, at]
            onward = jnp.dot(fade, up_to, precision=HIGHEST_MODE, preferred_element_type=jnp.float32)
            back = jnp.dot(fade, from_on, precision=HIGHEST_MODE, preferred_element_type=jnp.float32)
            cum = jnp.where(row_at < per_group, onward, back)
            stacked = jnp.concatenate(
                [cum, step, jnp.zeros((BLOCK - 2 * rows, BLOCK), jnp.float32)], axis=0
            )
            turned = jnp.transpose(stacked)
            cum_col, step_col = turned[:, 0:rows], turned[:, rows : 2 * rows]
            total = jnp.where(col_at < per_group, cum_col[BLOCK - 1 : BLOCK, :], cum_col[0:1, :])
            to_end = jnp.exp(total - cum_col) * step_col
            cum_scr[group, block] = cum
            col_scr[group, block] = cum_col
            x = conv_block(x_pad, x_taps, block, lanes_x)
            b = conv_block(b_pad, b_taps, block, lanes_s)
            x_kept[at, lanes_x] = x
            b_turned = jnp.transpose(b).astype(jnp.bfloat16)
            b_kept[group, block] = b_turned
            weighted = jnp.concatenate(
                [
                    x * spread_heads(to_end[:, 0:per_group], per_group),
                    x * spread_heads(to_end[:, per_group:rows], per_group),
                ],
                axis=1,
            ).astype(jnp.bfloat16)
            parts.append(jnp.dot(b_turned, weighted, preferred_element_type=jnp.float32))
            totals.append(total)
        for first, order in ((0, range(blocks)), (1, range(blocks - 1, -1, -1))):
            lanes = slice(first * width, (first + 1) * width)
            held = jnp.zeros((STATE, width), jnp.float32)
            for block in order:
                entry_scr[group, block, :, lanes] = held.astype(jnp.bfloat16)
                factor = spread_heads(
                    jnp.exp(totals[block][:, first * per_group : (first + 1) * per_group]), per_group
                )
                held = held * factor + parts[block][:, lanes]
            state_ref[first, group, 0:STATE, :] = held.astype(jnp.bfloat16)
            whole = totals[0]
            for block in range(1, blocks):
                whole = whole + totals[block]
            whole = spread_heads(
                jnp.exp(whole[:, first * per_group : (first + 1) * per_group]), per_group
            )
            state_ref[first, group, STATE:, :] = jnp.broadcast_to(
                whole, (state_ref.shape[2] - STATE, width)
            ).astype(jnp.bfloat16)
        for away in range(1, peers):
            state_copy(group, away).start()
        all_totals.append(totals)

    for group in range(groups):
        lanes_x = slice(group * width, (group + 1) * width)
        lanes_s = slice(group * STATE, (group + 1) * STATE)
        totals = all_totals[group]
        for block in range(blocks):
            at = slice(block * BLOCK, (block + 1) * BLOCK)
            step = fade_scr[group, rows : 2 * rows, at]
            cum, cum_col = cum_scr[group, block], col_scr[group, block]
            x = x_kept[at, lanes_x]
            c = conv_block(c_pad, c_taps, block, lanes_s).astype(jnp.bfloat16)
            c_kept[at, lanes_s] = c
            inner = jnp.dot(c, b_kept[group, block], preferred_element_type=jnp.float32)
            mixing = []
            for head in range(per_group):
                other = per_group + head
                gap = jnp.where(
                    i_at >= j_at,
                    cum_col[:, head : head + 1] - cum[head : head + 1, :],
                    cum_col[:, other : other + 1] - cum[other : other + 1, :],
                )
                own, opposite = step[head : head + 1, :], step[other : other + 1, :]
                amount = jnp.where(
                    i_at > j_at, own, jnp.where(i_at < j_at, opposite, own + opposite)
                )
                mixing.append((jnp.exp(gap) * amount * inner).astype(jnp.bfloat16))
            pieces = []
            for pair in range(per_group // 2):
                x_pair = x[:, pair * 2 * HEAD_DIM : (pair + 1) * 2 * HEAD_DIM]
                both = jnp.concatenate(
                    [jnp.where(half_lane, x_pair, 0.0), jnp.where(half_lane, 0.0, x_pair)], axis=0
                ).astype(jnp.bfloat16)
                left = jnp.concatenate([mixing[2 * pair], mixing[2 * pair + 1]], axis=1)
                pieces.append(jnp.dot(left, both, preferred_element_type=jnp.float32))
            readout = jnp.dot(c, entry_scr[group, block], preferred_element_type=jnp.float32)
            fade_in = jnp.exp(cum_col)
            y_ref[at, lanes_x] = (
                jnp.concatenate(pieces, axis=1)
                + readout[:, :width] * spread_heads(fade_in[:, 0:per_group], per_group)
                + readout[:, width:] * spread_heads(fade_in[:, per_group:rows], per_group)
            )
            offset = jnp.zeros((1, rows), jnp.float32)
            for earlier in range(blocks):
                if earlier < block:
                    offset = offset + jnp.where(col_at < per_group, totals[earlier], 0.0)
                if earlier > block:
                    offset = offset + jnp.where(col_at < per_group, 0.0, totals[earlier])
            reach_ref[group, at, :] = jnp.exp(cum_col + offset)

    def at_level(mask):
        return {"tp": 2 * flip(level, mask, levels) + core}

    def hand(mask):
        return remote(give.at[mask], take.at[mask], give_send.at[mask], take_recv.at[mask], partner)

    def post(mask):
        return remote(
            ship.at[mask], land.at[mask], ship_send.at[mask], land_recv.at[mask],
            at_level(low_bit(mask, levels)),
        )

    for load in loads:
        load.wait()
    for group in range(groups):
        for away in range(1, peers):
            state_copy(group, away).wait_recv()
        for first in range(2):
            held = jnp.zeros((STATE, width), jnp.float32)
            order = range(peers) if first == 0 else range(peers - 1, -1, -1)
            for peer in order:
                fresh = target[peer, group, 0:STATE, :].astype(jnp.float32)
                factor = target[peer, group, STATE : STATE + 1, :].astype(jnp.float32)
                reached = peer < here if first == 0 else peer > here
                held = jnp.where(reached, held * factor + fresh, held)
            carry_scr[group, :, first * width : (first + 1) * width] = held.astype(jnp.bfloat16)

    def gather(mask, lows):
        hand(mask).wait_recv()
        total = mine_scr[mask] + take[mask].astype(jnp.float32)
        for low in lows:
            post(mask + low).wait_recv()
            total = total + land[mask + low].astype(jnp.float32)
        return total

    def pass_on(mask, lows):
        ship[mask] = gather(mask, lows).astype(jnp.bfloat16)
        post(mask).start()

    def one_block(turn, _):
        mask = jnp.where(turn < levels // 2, levels - 1 - 2 * turn, 2 * levels - 2 - 2 * turn)
        at = pl.ds(pl.multiple_of(flip(level, mask, levels) * (2 * owned), 2 * owned), 2 * owned)
        mixed = []
        for group in range(groups):
            lanes = slice(group * width, (group + 1) * width)
            c = c_kept[at, group * STATE : (group + 1) * STATE]
            readout = jnp.dot(c, carry_scr[group], preferred_element_type=jnp.float32)
            reach = reach_ref[group, at, :]
            y = (
                y_ref[at, lanes]
                + readout[:, :width] * spread_heads(reach[:, 0:per_group], per_group)
                + readout[:, width:] * spread_heads(reach[:, per_group:rows], per_group)
            )
            gated = y * silu(gate_ref[at, lanes].astype(jnp.float32))
            square = jnp.mean(gated * gated, axis=-1, keepdims=True)
            mixed.append(
                (gated * lax.rsqrt(square + EPSILON) * gain_ref[:, lanes]).astype(jnp.bfloat16)
            )
        rows_mixed = mixed[0] if groups == 1 else jnp.concatenate(mixed, axis=1)
        tile = min(512, features)
        for start in range(0, features, tile):
            full_scr[:, start : start + tile] = jnp.dot(
                rows_mixed, weight_ref[:, start : start + tile], preferred_element_type=jnp.float32
            )
        own = pl.multiple_of(core * owned, owned)
        other = pl.multiple_of((1 - core) * owned, owned)
        give[mask] = full_scr[pl.ds(other, owned), :].astype(jnp.bfloat16)
        hand(mask).start()
        mine_scr[mask] = full_scr[pl.ds(own, owned), :]

        @pl.when((turn > 0) & (turn <= levels // 2))
        def _():
            pass_on(levels + 1 - 2 * turn, [])

        return 0

    lax.fori_loop(0, levels, one_block, 0)
    bits = [1 << n for n in range(levels.bit_length() - 1)]
    for bit in bits[1:]:
        for mask in range(levels - bit, 0, -2 * bit):
            pass_on(mask, [low for low in bits if low < bit])
    total = gather(0, bits)
    after = (skip_ref[...].astype(jnp.float32) + total).astype(jnp.bfloat16)
    after_ref[...] = after
    values = after.astype(jnp.float32)
    scale = lax.rsqrt(jnp.mean(values * values, axis=-1, keepdims=True) + EPSILON)
    normed_ref[...] = (values * scale * norm_gain_ref[...]).astype(jnp.bfloat16)
    for copy in route_copies:
        copy.wait_recv()

    def settle():
        for mask in range(levels):
            hand(mask).wait_send()
            if mask:
                post(mask).wait_send()
        for copy in route_copies:
            copy.wait_send()
        for group in range(groups):
            for away in range(1, peers):
                state_copy(group, away).wait_send()

        @pl.when(here < peers - 1)
        def _():
            for onward, _ in edges:
                onward.wait_send()

        @pl.when(here > 0)
        def _():
            for _, back in edges:
                back.wait_send()

    return settle


AHEAD = 2


def experts_part(
    normed_ref, after_ref, routes_ref, out_ref, loads, settle,
    rows_scr, stage, own_in, other_in, other_out, other_got, kept, hidden, returned,
    full_scr, mine_scr, give, take, ship, land, gate_w, up_w, down_w,
    row_send, row_recv, pair_send, pair_recv, out_send, out_recv, side_send, side_recv,
    sum_send, sum_recv, back_send, back_recv, give_send, take_recv, ship_send, land_recv,
):
    here, peers = lax.axis_index("sp"), lax.axis_size("sp")
    seat = lax.axis_index("tp")
    levels = lax.axis_size("tp") // 2
    core, level = seat % 2, seat // 2
    owned, features = normed_ref.shape
    share = stage.shape[2]
    slots = peers * share
    tokens = 2 * owned
    partner = {"tp": seat + 1 - 2 * core}
    away_order = list(range(peers - 1, 0, -1))

    def floor_of(mask):
        return flip(level, mask, levels)

    def at_level(mask):
        return {"tp": 2 * floor_of(mask) + core}

    def column(away):
        return flip(here, away, peers)

    def row_copy(mask):
        return remote(
            normed_ref, rows_scr.at[level, core], row_send.at[mask], row_recv.at[mask],
            at_level(mask),
        )

    def pair_copy(mask):
        spot = rows_scr.at[floor_of(mask), core]
        source = normed_ref if isinstance(mask, int) and mask == 0 else spot
        return remote(source, spot, pair_send.at[mask], pair_recv.at[mask], partner)

    def out_copy(mask, away):
        floor = floor_of(mask)
        return remote(
            stage.at[floor, column(away)], own_in.at[floor, here],
            out_send.at[mask, away], out_recv.at[mask, away], {"sp": column(away)},
        )

    def side_copy(mask, away):
        return remote(
            own_in.at[floor_of(mask), column(away)], other_in.at[mask % 2, column(away)],
            side_send.at[mask, away], side_recv.at[mask, away], partner,
        )

    def sum_copy(mask):
        return remote(
            other_out.at[mask % 2], other_got.at[mask % 2], sum_send.at[mask], sum_recv.at[mask],
            partner,
        )

    def back_copy(mask, away):
        floor = floor_of(mask)
        return remote(
            stage.at[floor, column(away)], returned.at[floor, here],
            back_send.at[mask, away], back_recv.at[mask, away], {"sp": column(away)},
        )

    def hand(mask):
        return remote(give.at[mask], take.at[mask], give_send.at[mask], take_recv.at[mask], partner)

    def post(mask):
        return remote(
            ship.at[mask], land.at[mask], ship_send.at[mask], land_recv.at[mask], at_level(mask)
        )

    rows_scr[level, core] = normed_ref[...]
    for mask in range(1, levels):
        row_copy(mask).start()

    def routes_of(mask):
        floor = floor_of(mask)
        return routes_ref[2 * floor] + routes_ref[2 * floor + 1]

    def dispatch(mask):
        floor = floor_of(mask)
        pair_copy(mask).start()
        tile = routes_of(mask)
        code = (
            lax.broadcasted_iota(jnp.int32, (slots, tokens), 0) + core * slots
        ).astype(jnp.float32)
        chosen = (tile[0:1, 0:tokens] == code) | (tile[1:2, 0:tokens] == code)
        chosen = jnp.where(chosen, 1.0, 0.0).astype(jnp.bfloat16)
        pair_copy(mask).wait_recv()
        width = min(512, features)
        for start in range(0, features, width):
            lanes = slice(start, start + width)
            rows = rows_scr[floor, :, :, lanes].reshape(tokens, width)
            picked = jnp.dot(chosen, rows, preferred_element_type=jnp.float32)
            stage[floor, :, :, lanes] = picked.astype(jnp.bfloat16).reshape(peers, share, width)
        own_in[floor, here] = stage[floor, here]
        for away in away_order:
            out_copy(mask, away).start()

    def arrive_and_dispatch(mask):
        row_copy(mask).wait_recv()
        dispatch(mask)

    dispatch(0)
    for mask in range(1, min(AHEAD, levels)):
        arrive_and_dispatch(mask)
    for load in loads:
        load.wait()

    def expert(index, source, store):
        hid = gate_w.shape[2]
        width = min(256, hid)

        def up_tile(n, _):
            lanes = pl.ds(pl.multiple_of(n * width, width), width)
            x = source[...].reshape(slots, features)
            gate = jnp.dot(x, gate_w[index, :, lanes], preferred_element_type=jnp.float32)
            up = jnp.dot(x, up_w[index, :, lanes], preferred_element_type=jnp.float32)
            hidden[:, lanes] = (silu(gate) * up).astype(jnp.bfloat16)
            return 0

        lax.fori_loop(0, hid // width, up_tile, 0)
        wide = min(512, features)

        def down_tile(n, _):
            lanes = pl.ds(pl.multiple_of(n * wide, wide), wide)
            store(
                lanes,
                jnp.dot(hidden[...], down_w[index, :, lanes], preferred_element_type=jnp.float32),
            )
            return 0

        lax.fori_loop(0, features // wide, down_tile, 0)

    def one_floor(mask, _):
        floor = floor_of(mask)
        side_copy(mask, 0).start()
        for away in away_order:
            out_copy(mask, away).wait_recv()
            side_copy(mask, away).start()
        if AHEAD < levels:

            @pl.when(mask + AHEAD < levels)
            def _():
                arrive_and_dispatch(mask + AHEAD)

        for away in range(peers):
            side_copy(mask, away).wait_recv()

        @pl.when(mask >= 2)
        def _():
            sum_copy(mask - 2).wait_send()

        def give_out(lanes, value):
            other_out[mask % 2, :, lanes] = value.astype(jnp.bfloat16)

        def keep(lanes, value):
            kept[:, lanes] = value

        expert(1 - core, other_in.at[mask % 2], give_out)
        sum_copy(mask).start()
        expert(core, own_in.at[floor], keep)
        for away in away_order:
            out_copy(mask, away).wait_send()
        sum_copy(mask).wait_recv()
        both = (kept[...] + other_got[mask % 2].astype(jnp.float32)).astype(jnp.bfloat16)
        stage[floor] = both.reshape(peers, share, features)
        returned[floor, here] = stage[floor, here]

        @pl.when(mask >= levels // 2)
        def _():
            for away in away_order:
                back_copy(mask, away).start()

        return 0

    lax.fori_loop(0, levels, one_floor, 0)
    for mask in range(levels // 2 - 1, -1, -1):
        for away in away_order:
            back_copy(mask, away).start()

    def turn_mask(turn):
        return jnp.where(turn < levels // 2, turn + levels // 2, levels - 1 - turn)

    def pass_on(mask):
        hand(mask).wait_recv()
        ship[mask] = (mine_scr[mask] + take[mask].astype(jnp.float32)).astype(jnp.bfloat16)
        post(mask).start()

    def combine(turn, _):
        mask = turn_mask(turn)
        tile = routes_of(mask)
        size = tile.shape[1]
        turned = jnp.transpose(
            jnp.concatenate([tile, jnp.zeros((size - tile.shape[0], size), jnp.float32)], axis=0)
        )[0:tokens, :]
        code = (
            lax.broadcasted_iota(jnp.int32, (tokens, slots), 1) + core * slots
        ).astype(jnp.float32)
        weight = jnp.where(turned[:, 0:1] == code, turned[:, 2:3], 0.0) + jnp.where(
            turned[:, 1:2] == code, turned[:, 3:4], 0.0
        )
        high = weight.astype(jnp.bfloat16)
        low = (weight - high.astype(jnp.float32)).astype(jnp.bfloat16)
        for away in away_order:
            back_copy(mask, away).wait_recv()
        width = min(512, features)
        for start in range(0, features, width):
            lanes = slice(start, start + width)
            got = returned[floor_of(mask), :, :, lanes].reshape(slots, width)
            full_scr[:, lanes] = jnp.dot(
                high, got, preferred_element_type=jnp.float32
            ) + jnp.dot(low, got, preferred_element_type=jnp.float32)
        own = pl.multiple_of(core * owned, owned)
        other = pl.multiple_of((1 - core) * owned, owned)
        give[mask] = full_scr[pl.ds(other, owned), :].astype(jnp.bfloat16)
        hand(mask).start()
        mine_scr[mask] = full_scr[pl.ds(own, owned), :]

        @pl.when(turn > 0)
        def _():
            pass_on(turn_mask(turn - 1))

        return 0

    settle()
    lax.fori_loop(0, levels, combine, 0)
    hand(0).wait_recv()
    total = mine_scr[0] + take[0].astype(jnp.float32)
    for mask in range(1, levels):
        post(mask).wait_recv()
        total = total + land[mask].astype(jnp.float32)
    out_ref[...] = after_ref[...].astype(jnp.float32) + total

    for mask in range(levels):
        pair_copy(mask).wait_send()
        hand(mask).wait_send()
        if mask:
            row_copy(mask).wait_send()
            post(mask).wait_send()
        if mask + 2 >= levels:
            sum_copy(mask).wait_send()
        for away in range(peers):
            side_copy(mask, away).wait_send()
            if away:
                back_copy(mask, away).wait_send()


def layer_kernel(experts_here, share, counts, *refs):
    refs = list(refs)

    def take(number):
        out = refs[:number]
        del refs[:number]
        return out

    near = take(counts[0])
    far = take(counts[1])
    (out_ref,) = take(1)
    loaded = take(counts[1])
    after_ref, normed_ref, routes = take(3)
    mixer_own = take(counts[2])
    shared = take(6)
    mixer_flags = take(10)
    experts_own = take(9)
    experts_flags = take(16)
    (load_sem,) = take(1)
    loads = [
        pltpu.make_async_copy(source, target, load_sem.at[index])
        for index, (source, target) in enumerate(zip(far, loaded))
    ]
    for load in loads:
        load.start()
    here, peers = lax.axis_index("sp"), lax.axis_size("sp")
    seat, seats = lax.axis_index("tp"), lax.axis_size("tp")
    greet(
        [{"sp": lax.rem(here + away, peers)} for away in range(1, peers)]
        + [{"tp": lax.rem(seat + away, seats)} for away in range(1, seats)]
    )
    settle = mixer_part(
        *near, *loaded[0:3], loads[0:3], after_ref, normed_ref, routes, experts_here, share,
        *mixer_own, *shared, *mixer_flags,
    )
    experts_part(
        normed_ref, after_ref, routes, out_ref, loads[3:], settle,
        *experts_own, *shared, *loaded[3:], *experts_flags,
    )


def per_device(
    skip_stream_entry,
    result_switch_mapped,
    channel_feed_mapped,
    write_coefficient_mapped,
    emission_coefficient_mapped,
    channel_feed_taps,
    write_coefficient_taps,
    emission_coefficient_taps,
    raw_increments,
    channel_log_fade_speed,
    extra_log_fade,
    cluster_scaling_factor,
    blend_result_matrix,
    routing_scaling_factor,
    specialist_switch_matrix,
    specialist_widen_matrix,
    specialist_contract_matrix,
    picked_specialists,
    router_affinities,
):
    count, inner_here = channel_feed_mapped.shape
    owned, features = skip_stream_entry.shape
    experts_here, _, units = specialist_switch_matrix.shape
    peers, seats = lax.axis_size("sp"), lax.axis_size("tp")
    levels = seats // 2
    groups = write_coefficient_mapped.shape[1] // STATE
    width = inner_here // groups
    rows = 2 * (width // HEAD_DIM)
    blocks = count // BLOCK
    depth = STATE + 16
    capacity = max(2, 3 * TOP * owned // (2 * experts_here * peers))
    share = 2 * (-(-capacity // 8) * 8)
    slots = peers * share
    vmem, anywhere = pl.BlockSpec(memory_space=pltpu.VMEM), pl.BlockSpec(memory_space=pl.ANY)

    def half(*shape):
        return pltpu.VMEM(shape, jnp.bfloat16)

    def full(*shape):
        return pltpu.VMEM(shape, jnp.float32)

    def flags(*shape):
        return pltpu.SemaphoreType.DMA(shape)

    near = [
        channel_feed_mapped, write_coefficient_mapped, emission_coefficient_mapped,
        channel_feed_taps, write_coefficient_taps, emission_coefficient_taps, raw_increments,
        channel_log_fade_speed, extra_log_fade, picked_specialists.T, router_affinities.T,
        cluster_scaling_factor.reshape(1, -1), routing_scaling_factor.reshape(1, -1),
    ]
    far = [
        result_switch_mapped, skip_stream_entry, blend_result_matrix,
        specialist_switch_matrix, specialist_widen_matrix, specialist_contract_matrix,
    ]
    lines = groups * STATE
    mixer_own = [
        full(count + 2 * RIM, inner_here), full(count + 2 * RIM, lines), full(count + 2 * RIM, lines),
        half(EDGE, inner_here), half(EDGE, lines), half(EDGE, lines),
        half(EDGE, inner_here), half(EDGE, lines), half(EDGE, lines),
        full(groups, 2 * rows, count), full(count, inner_here), half(groups, blocks, STATE, BLOCK),
        half(count, lines), full(groups, blocks, rows, BLOCK), full(groups, blocks, BLOCK, rows),
        half(groups, blocks, STATE, 2 * width), half(2, groups, depth, width),
        half(peers, groups, depth, width), full(count, inner_here), full(groups, count, rows),
        half(groups, STATE, 2 * width), full(8, 128),
    ]
    slab = (levels, owned, features)
    shared = [full(2 * owned, features), full(*slab)] + [half(*slab)] * 4
    mixer_flags = [
        flags(2, 3), flags(2, 3), flags(groups, peers - 1), flags(groups, peers - 1),
        flags(seats - 1), flags(seats - 1), flags(levels), flags(levels), flags(levels), flags(levels),
    ]
    experts_own = [
        half(levels, 2, owned, features),
        half(levels, peers, share, features),
        half(levels, peers, share, features),
        half(2, peers, share, features),
        half(2, slots, features),
        half(2, slots, features),
        full(slots, features),
        half(slots, units),
        half(levels, peers, share, features),
    ]
    experts_flags = [
        flags(levels), flags(levels), flags(levels), flags(levels),
        flags(levels, peers), flags(levels, peers), flags(levels, peers), flags(levels, peers),
        flags(levels), flags(levels), flags(levels, peers), flags(levels, peers),
        flags(levels), flags(levels), flags(levels), flags(levels),
    ]
    return pl.pallas_call(
        functools.partial(layer_kernel, experts_here, share, (len(near), len(far), len(mixer_own))),
        in_specs=[vmem] * len(near) + [anywhere] * len(far),
        out_specs=vmem,
        out_shape=jax.ShapeDtypeStruct((owned, features), jnp.float32),
        scratch_shapes=[half(*array.shape) for array in far]
        + [half(owned, features), half(owned, features), full(seats, 8, 128)]
        + mixer_own + shared + mixer_flags + experts_own + experts_flags + [flags(len(far))],
        compiler_params=pltpu.CompilerParams(
            collective_id=0, has_side_effects=True, vmem_limit_bytes=67043328
        ),
        name="layer",
    )(*near, *far).astype(jnp.bfloat16)


def solution(mesh):
    in_specs = (
        P(("sp", "tp"), None),
        P("sp", "tp"),
        P("sp", "tp"),
        P("sp", "tp"),
        P("sp", "tp"),
        P(None, "tp"),
        P(None, "tp"),
        P(None, "tp"),
        P(None, "tp", "sp"),
        P(None, "tp"),
        P(None, "tp", "sp"),
        P("tp"),
        P("tp", None),
        P(),
        P("sp", None, "tp"),
        P("sp", None, "tp"),
        P("sp", "tp", None),
        P(("sp", "tp"), None),
        P(("sp", "tp"), None),
    )
    out_specs = P(("sp", "tp"), None)
    return jax.shard_map(
        per_device, mesh=mesh, in_specs=in_specs, out_specs=out_specs, check_vma=False
    )
```

```python
import functools

import jax
import jax.numpy as jnp
from jax import lax
from jax.experimental import pallas as pl
from jax.experimental.pallas import tpu as pltpu
from jax.sharding import PartitionSpec as P

WIDTH = 2048
HEAD_DIM = 64
GROUPS = 16
STATE = 128
CONV_W = 5
BLOCK = 128
TOP = 2
INNER = 4096


EPSILON = 1e-06
HIGHEST_MODE = lax.Precision.HIGHEST


MESH_IDS = pl.DeviceIdType.MESH
RIM = 8
EDGE = 16


def spread_heads(columns, per_group):
    rows = columns.shape[0]
    lane = lax.broadcasted_iota(jnp.int32, (rows, per_group * HEAD_DIM), 1) // HEAD_DIM
    out = jnp.broadcast_to(columns[:, 0:1], lane.shape)
    for head in range(1, per_group):
        out = jnp.where(lane == head, jnp.broadcast_to(columns[:, head : head + 1], lane.shape), out)
    return out


def silu(value):
    return value * jax.nn.sigmoid(value)


def conv_block(scratch, taps, block, lanes):
    rim = taps.shape[0] // 2
    total = None
    for offset in range(taps.shape[0]):
        start = RIM - rim + offset + block * BLOCK
        term = taps[offset : offset + 1, lanes].astype(jnp.float32) * scratch[start : start + BLOCK, lanes]
        total = term if total is None else total + term
    return silu(total)


def flip(index, mask, count):
    out, bit = index, 1
    while bit < count:
        out = out + ((mask // bit) % 2) * (1 - 2 * ((index // bit) % 2)) * bit
        bit = 2 * bit
    return out


def low_bit(mask, count):
    out, bit = 0, count // 2
    while bit >= 1:
        odd = (mask // bit) % 2
        out = odd * bit + (1 - odd) * out
        bit = bit // 2
    return out


def remote(source, target, send_sem, recv_sem, where):
    return pltpu.make_async_remote_copy(
        src_ref=source, dst_ref=target, send_sem=send_sem, recv_sem=recv_sem,
        device_id=where, device_id_type=MESH_IDS,
    )


def greet(places):
    barrier = pltpu.get_barrier_semaphore()
    for place in places:
        pl.semaphore_signal(barrier, inc=1, device_id=place, device_id_type=MESH_IDS)
    pl.semaphore_wait(barrier, len(places))


def write_route(picks_ref, affinity_ref, route_scr, experts_here, share):
    owned = picks_ref.shape[1]
    peers, core = lax.axis_size("sp"), lax.axis_index("tp") % 2
    picks, affinity = picks_ref[...], affinity_ref[...]
    count = -(-experts_here * peers // 8) * 8
    expert = lax.broadcasted_iota(jnp.int32, (count, owned), 0)
    marks = [jnp.where(picks[k : k + 1, :] == expert, 1.0, 0.0) for k in range(TOP)]
    earlier = jnp.where(
        lax.broadcasted_iota(jnp.int32, (owned, owned), 0)
        < lax.broadcasted_iota(jnp.int32, (owned, owned), 1),
        1.0,
        0.0,
    ).astype(jnp.bfloat16)
    ahead = jnp.dot(
        (marks[0] + marks[1]).astype(jnp.bfloat16), earlier, preferred_element_type=jnp.float32
    )
    base = (expert % experts_here) * (peers * share) + (expert // experts_here) * share
    base = (base + core * (share // 2)).astype(jnp.float32) + ahead
    places = [jnp.sum(mark * base, axis=0, keepdims=True) for mark in marks]
    whole = affinity[0:1, :] + affinity[1:2, :]
    lines = jnp.concatenate(
        places
        + [affinity[0:1, :] / whole, affinity[1:2, :] / whole]
        + [jnp.zeros((8 - 2 * TOP, owned), jnp.float32)],
        axis=0,
    )
    blank = jnp.zeros_like(lines)
    rest = [] if 2 * owned == 128 else [jnp.zeros((8, 128 - 2 * owned), jnp.float32)]
    route_scr[...] = jnp.concatenate(
        [jnp.where(core == 0, lines, blank), jnp.where(core == 0, blank, lines)] + rest, axis=1
    )


def mixer_part(
    x_ref, b_ref, c_ref, x_taps, b_taps, c_taps, inc_ref, speed_ref, extra_ref, picks_ref,
    affinity_ref, gain_ref, norm_gain_ref, gate_ref, skip_ref, weight_ref, loads, after_ref,
    normed_ref, routes, experts_here, share,
    x_pad, b_pad, c_pad, x_low, b_low, c_low, x_high, b_high, c_high, fade_scr, x_kept, b_kept,
    c_kept, cum_scr, col_scr, entry_scr, state_ref, target, y_ref, reach_ref, carry_scr, route_scr,
    full_scr, mine_scr, give, take, ship, land,
    edge_send, edge_recv, state_send, state_recv, route_send, route_recv,
    give_send, take_recv, ship_send, land_recv,
):
    count, inner_here = x_ref.shape
    groups = b_ref.shape[1] // STATE
    width = inner_here // groups
    per_group = width // HEAD_DIM
    rows = 2 * per_group
    blocks = count // BLOCK
    rim = x_taps.shape[0] // 2
    here, peers = lax.axis_index("sp"), lax.axis_size("sp")
    seat, seats = lax.axis_index("tp"), lax.axis_size("tp")
    levels = seats // 2
    core, level = seat % 2, seat // 2
    owned, features = skip_ref.shape
    partner = {"tp": seat + 1 - 2 * core}

    edges = []
    for index, (source, low, high) in enumerate(
        ((x_ref, x_low, x_high), (b_ref, b_low, b_high), (c_ref, c_low, c_high))
    ):
        onward = remote(
            source.at[pl.ds(count - EDGE, EDGE)], low, edge_send.at[0, index],
            edge_recv.at[0, index], {"sp": lax.rem(here + 1, peers)},
        )
        back = remote(
            source.at[pl.ds(0, EDGE)], high, edge_send.at[1, index],
            edge_recv.at[1, index], {"sp": lax.rem(here + peers - 1, peers)},
        )
        edges.append((onward, back))

    @pl.when(here < peers - 1)
    def _():
        for onward, _ in edges:
            onward.start()

    @pl.when(here > 0)
    def _():
        for _, back in edges:
            back.start()

    write_route(picks_ref, affinity_ref, route_scr, experts_here, share)
    route_copies = [
        remote(
            route_scr, routes.at[seat], route_send.at[away - 1], route_recv.at[away - 1],
            {"tp": lax.rem(seat + away, seats)},
        )
        for away in range(1, seats)
    ]
    for copy in route_copies:
        copy.start()
    routes[seat] = route_scr[...]
    target[here] = jnp.zeros(target.shape[1:], target.dtype)

    heads = inc_ref.shape[1]
    square_at = [lax.broadcasted_iota(jnp.int32, (heads, heads), axis) for axis in range(2)]
    for first in range(2):
        raw = inc_ref[first].astype(jnp.float32)
        step = jnp.maximum(raw, 0.0) + jnp.log1p(jnp.exp(-jnp.abs(raw)))
        line = jnp.broadcast_to(speed_ref[first : first + 1, :], (heads, heads))
        speed = jnp.sum(
            jnp.where(square_at[0] == square_at[1], jnp.exp(line), 0.0), axis=1, keepdims=True
        )
        fade = -step * speed + extra_ref[first]
        for group in range(groups):
            mine = slice(group * per_group, (group + 1) * per_group)
            spot = first * per_group
            fade_scr[group, spot : spot + per_group, :] = fade[mine, :]
            fade_scr[group, rows + spot : rows + spot + per_group, :] = step[mine, :]
    for pad, source in ((x_pad, x_ref), (b_pad, b_ref), (c_pad, c_ref)):
        pad[RIM : RIM + count, :] = source[...].astype(jnp.float32)

    @pl.when(here > 0)
    def _():
        for onward, _ in edges:
            onward.wait_recv()
        for pad, low in ((x_pad, x_low), (b_pad, b_low), (c_pad, c_low)):
            pad[RIM - rim : RIM, :] = low[...].astype(jnp.float32)[EDGE - rim : EDGE, :]

    @pl.when(here == 0)
    def _():
        for pad in (x_pad, b_pad, c_pad):
            pad[RIM - rim : RIM, :] = jnp.zeros((rim, pad.shape[1]), jnp.float32)

    @pl.when(here < peers - 1)
    def _():
        for _, back in edges:
            back.wait_recv()
        for pad, high in ((x_pad, x_high), (b_pad, b_high), (c_pad, c_high)):
            pad[RIM + count : RIM + count + rim, :] = high[...].astype(jnp.float32)[0:rim, :]

    @pl.when(here == peers - 1)
    def _():
        for pad in (x_pad, b_pad, c_pad):
            pad[RIM + count : RIM + count + rim, :] = jnp.zeros((rim, pad.shape[1]), jnp.float32)

    i_at = lax.broadcasted_iota(jnp.int32, (BLOCK, BLOCK), 0)
    j_at = lax.broadcasted_iota(jnp.int32, (BLOCK, BLOCK), 1)
    up_to = (i_at <= j_at).astype(jnp.float32)
    from_on = (i_at >= j_at).astype(jnp.float32)
    col_at = lax.broadcasted_iota(jnp.int32, (1, rows), 1)
    half_lane = lax.broadcasted_iota(jnp.int32, (BLOCK, 2 * HEAD_DIM), 1) < HEAD_DIM

    def state_copy(group, away):
        peer = lax.rem(here + away, peers)
        return remote(
            state_ref.at[jnp.where(peer > here, 0, 1), group], target.at[here, group],
            state_send.at[group, away - 1], state_recv.at[group, away - 1], {"sp": peer},
        )

    spots = [(group, block) for group in range(groups) for block in range(blocks)]
    fades = jnp.concatenate(
        [fade_scr[g, 0:rows, b * BLOCK : (b + 1) * BLOCK] for g, b in spots], axis=0
    )
    onward = jnp.dot(fades, up_to, precision=HIGHEST_MODE, preferred_element_type=jnp.float32)
    back = jnp.dot(fades, from_on, precision=HIGHEST_MODE, preferred_element_type=jnp.float32)
    row_at = lax.broadcasted_iota(jnp.int32, fades.shape, 0)
    sums = jnp.where(row_at % rows < per_group, onward, back)
    lines, columns, per_turn = [], {}, BLOCK // (2 * rows)
    for index, (g, b) in enumerate(spots):
        cum = sums[index * rows : (index + 1) * rows, :]
        cum_scr[g, b] = cum
        lines += [cum, fade_scr[g, rows : 2 * rows, b * BLOCK : (b + 1) * BLOCK]]
    for start in range(0, len(spots), per_turn):
        part = lines[2 * start : 2 * (start + per_turn)]
        rest = BLOCK - rows * len(part)
        if rest:
            part = part + [jnp.zeros((rest, BLOCK), jnp.float32)]
        turned = jnp.transpose(jnp.concatenate(part, axis=0))
        for offset, spot in enumerate(spots[start : start + per_turn]):
            lane = 2 * rows * offset
            columns[spot] = (
                turned[:, lane : lane + rows], turned[:, lane + rows : lane + 2 * rows]
            )

    all_totals = []
    for group in range(groups):
        lanes_x = slice(group * width, (group + 1) * width)
        lanes_s = slice(group * STATE, (group + 1) * STATE)
        totals, parts = [], []
        for block in range(blocks):
            at = slice(block * BLOCK, (block + 1) * BLOCK)
            cum_col, step_col = columns[group, block]
            total = jnp.where(col_at < per_group, cum_col[BLOCK - 1 : BLOCK, :], cum_col[0:1, :])
            to_end = jnp.exp(total - cum_col) * step_col
            col_scr[group, block] = cum_col
            x = conv_block(x_pad, x_taps, block, lanes_x)
            b = conv_block(b_pad, b_taps, block, lanes_s)
            x_kept[at, lanes_x] = x
            b_turned = jnp.transpose(b).astype(jnp.bfloat16)
            b_kept[group, block] = b_turned
            weighted = jnp.concatenate(
                [
                    x * spread_heads(to_end[:, 0:per_group], per_group),
                    x * spread_heads(to_end[:, per_group:rows], per_group),
                ],
                axis=1,
            ).astype(jnp.bfloat16)
            parts.append(jnp.dot(b_turned, weighted, preferred_element_type=jnp.float32))
            totals.append(total)
        for first, order in ((0, range(blocks)), (1, range(blocks - 1, -1, -1))):
            lanes = slice(first * width, (first + 1) * width)
            held = jnp.zeros((STATE, width), jnp.float32)
            for block in order:
                entry_scr[group, block, :, lanes] = held.astype(jnp.bfloat16)
                factor = spread_heads(
                    jnp.exp(totals[block][:, first * per_group : (first + 1) * per_group]), per_group
                )
                held = held * factor + parts[block][:, lanes]
            state_ref[first, group, 0:STATE, :] = held.astype(jnp.bfloat16)
            whole = totals[0]
            for block in range(1, blocks):
                whole = whole + totals[block]
            whole = spread_heads(
                jnp.exp(whole[:, first * per_group : (first + 1) * per_group]), per_group
            )
            state_ref[first, group, STATE:, :] = jnp.broadcast_to(
                whole, (state_ref.shape[2] - STATE, width)
            ).astype(jnp.bfloat16)
        for away in range(1, peers):
            state_copy(group, away).start()
        all_totals.append(totals)

    for group in range(groups):
        lanes_s = slice(group * STATE, (group + 1) * STATE)
        totals = all_totals[group]
        for block in range(blocks):
            at = slice(block * BLOCK, (block + 1) * BLOCK)
            c_kept[at, lanes_s] = conv_block(c_pad, c_taps, block, lanes_s).astype(jnp.bfloat16)
            offset = jnp.zeros((1, rows), jnp.float32)
            for earlier in range(blocks):
                if earlier < block:
                    offset = offset + jnp.where(col_at < per_group, totals[earlier], 0.0)
                if earlier > block:
                    offset = offset + jnp.where(col_at < per_group, 0.0, totals[earlier])
            reach_ref[group, at, :] = jnp.exp(col_scr[group, block] + offset)

    def within(block):
        at = pl.ds(pl.multiple_of(block * BLOCK, BLOCK), BLOCK)
        for group in range(groups):
            lanes_x = slice(group * width, (group + 1) * width)
            lanes_s = slice(group * STATE, (group + 1) * STATE)
            step = fade_scr[group, rows : 2 * rows, at]
            cum, cum_col = cum_scr[group, block], col_scr[group, block]
            x = x_kept[at, lanes_x]
            c = c_kept[at, lanes_s]
            inner = jnp.dot(c, b_kept[group, block], preferred_element_type=jnp.float32)
            mixing = []
            for head in range(per_group):
                other = per_group + head
                gap = jnp.where(
                    i_at >= j_at,
                    cum_col[:, head : head + 1] - cum[head : head + 1, :],
                    cum_col[:, other : other + 1] - cum[other : other + 1, :],
                )
                own, opposite = step[head : head + 1, :], step[other : other + 1, :]
                amount = jnp.where(
                    i_at > j_at, own, jnp.where(i_at < j_at, opposite, own + opposite)
                )
                mixing.append((jnp.exp(gap) * amount * inner).astype(jnp.bfloat16))
            pieces = []
            for pair in range(per_group // 2):
                x_pair = x[:, pair * 2 * HEAD_DIM : (pair + 1) * 2 * HEAD_DIM]
                both = jnp.concatenate(
                    [jnp.where(half_lane, x_pair, 0.0), jnp.where(half_lane, 0.0, x_pair)], axis=0
                ).astype(jnp.bfloat16)
                left = jnp.concatenate([mixing[2 * pair], mixing[2 * pair + 1]], axis=1)
                pieces.append(jnp.dot(left, both, preferred_element_type=jnp.float32))
            readout = jnp.dot(c, entry_scr[group, block], preferred_element_type=jnp.float32)
            fade_in = jnp.exp(cum_col)
            y_ref[at, lanes_x] = (
                jnp.concatenate(pieces, axis=1)
                + readout[:, :width] * spread_heads(fade_in[:, 0:per_group], per_group)
                + readout[:, width:] * spread_heads(fade_in[:, per_group:rows], per_group)
            )

    def at_level(mask):
        return {"tp": 2 * flip(level, mask, levels) + core}

    def hand(mask):
        return remote(give.at[mask], take.at[mask], give_send.at[mask], take_recv.at[mask], partner)

    def post(mask):
        return remote(
            ship.at[mask], land.at[mask], ship_send.at[mask], land_recv.at[mask],
            at_level(low_bit(mask, levels)),
        )

    def block_mask(turn):
        return jnp.where(turn < levels // 2, levels - 1 - 2 * turn, 2 * levels - 2 - 2 * turn)

    woven = 2 * owned == BLOCK and blocks == levels
    early = min(2, levels) if woven else blocks

    def first_blocks(turn, _):
        within(flip(level, block_mask(turn), levels) if woven else turn)
        return 0

    lax.fori_loop(0, early, first_blocks, 0)
    for load in loads:
        load.wait()
    for group in range(groups):
        for away in range(1, peers):
            state_copy(group, away).wait_recv()
        for first in range(2):
            held = jnp.zeros((STATE, width), jnp.float32)
            order = range(peers) if first == 0 else range(peers - 1, -1, -1)
            for peer in order:
                fresh = target[peer, group, 0:STATE, :].astype(jnp.float32)
                factor = target[peer, group, STATE : STATE + 1, :].astype(jnp.float32)
                reached = peer < here if first == 0 else peer > here
                held = jnp.where(reached, held * factor + fresh, held)
            carry_scr[group, :, first * width : (first + 1) * width] = held.astype(jnp.bfloat16)

    def gather(mask, lows):
        hand(mask).wait_recv()
        total = mine_scr[mask] + take[mask].astype(jnp.float32)
        for low in lows:
            post(mask + low).wait_recv()
            total = total + land[mask + low].astype(jnp.float32)
        return total

    def pass_on(mask, lows):
        ship[mask] = gather(mask, lows).astype(jnp.bfloat16)
        post(mask).start()

    def one_block(turn, _):
        mask = block_mask(turn)
        at = pl.ds(pl.multiple_of(flip(level, mask, levels) * (2 * owned), 2 * owned), 2 * owned)
        mixed = []
        for group in range(groups):
            lanes = slice(group * width, (group + 1) * width)
            c = c_kept[at, group * STATE : (group + 1) * STATE]
            readout = jnp.dot(c, carry_scr[group], preferred_element_type=jnp.float32)
            reach = reach_ref[group, at, :]
            y = (
                y_ref[at, lanes]
                + readout[:, :width] * spread_heads(reach[:, 0:per_group], per_group)
                + readout[:, width:] * spread_heads(reach[:, per_group:rows], per_group)
            )
            gated = y * silu(gate_ref[at, lanes].astype(jnp.float32))
            square = jnp.mean(gated * gated, axis=-1, keepdims=True)
            mixed.append(
                (gated * lax.rsqrt(square + EPSILON) * gain_ref[:, lanes]).astype(jnp.bfloat16)
            )
        rows_mixed = mixed[0] if groups == 1 else jnp.concatenate(mixed, axis=1)
        tile = min(512, features)
        for start in range(0, features, tile):
            full_scr[:, start : start + tile] = jnp.dot(
                rows_mixed, weight_ref[:, start : start + tile], preferred_element_type=jnp.float32
            )
        own = pl.multiple_of(core * owned, owned)
        other = pl.multiple_of((1 - core) * owned, owned)
        give[mask] = full_scr[pl.ds(other, owned), :].astype(jnp.bfloat16)
        hand(mask).start()
        mine_scr[mask] = full_scr[pl.ds(own, owned), :]

        if woven:

            @pl.when(turn + early < levels)
            def _():
                within(flip(level, block_mask(turn + early), levels))

        @pl.when(turn < levels // 2)
        def _():
            pass_on(mask, [])

        return 0

    lax.fori_loop(0, levels, one_block, 0)
    bits = [1 << n for n in range(levels.bit_length() - 1)]
    for bit in bits[1:]:
        for mask in range(levels - bit, 0, -2 * bit):
            pass_on(mask, [low for low in bits if low < bit])
    total = gather(0, bits)
    after = (skip_ref[...].astype(jnp.float32) + total).astype(jnp.bfloat16)
    after_ref[...] = after
    values = after.astype(jnp.float32)
    scale = lax.rsqrt(jnp.mean(values * values, axis=-1, keepdims=True) + EPSILON)
    normed_ref[...] = (values * scale * norm_gain_ref[...]).astype(jnp.bfloat16)
    for copy in route_copies:
        copy.wait_recv()

    def settle():
        for mask in range(levels):
            hand(mask).wait_send()
            if mask:
                post(mask).wait_send()
        for copy in route_copies:
            copy.wait_send()
        for group in range(groups):
            for away in range(1, peers):
                state_copy(group, away).wait_send()

        @pl.when(here < peers - 1)
        def _():
            for onward, _ in edges:
                onward.wait_send()

        @pl.when(here > 0)
        def _():
            for _, back in edges:
                back.wait_send()

    return settle


AHEAD = 2


def experts_part(
    normed_ref, after_ref, routes_ref, out_ref, loads, settle,
    rows_scr, stage, own_in, other_in, other_out, other_got, kept, hidden, returned,
    full_scr, mine_scr, give, take, ship, land, gate_w, up_w, down_w,
    row_send, row_recv, pair_send, pair_recv, out_send, out_recv, side_send, side_recv,
    sum_send, sum_recv, back_send, back_recv, give_send, take_recv, ship_send, land_recv,
):
    here, peers = lax.axis_index("sp"), lax.axis_size("sp")
    seat = lax.axis_index("tp")
    levels = lax.axis_size("tp") // 2
    core, level = seat % 2, seat // 2
    owned, features = normed_ref.shape
    share = stage.shape[2]
    slots = peers * share
    tokens = 2 * owned
    partner = {"tp": seat + 1 - 2 * core}
    away_order = list(range(peers - 1, 0, -1))

    def floor_of(mask):
        return flip(level, mask, levels)

    def at_level(mask):
        return {"tp": 2 * floor_of(mask) + core}

    def column(away):
        return flip(here, away, peers)

    bits = [1 << n for n in range(levels.bit_length() - 1)]

    def row_copy(mask):
        low = low_bit(mask, levels)
        spot = rows_scr.at[floor_of(mask - low), core]
        source = normed_ref if isinstance(mask, int) and mask in bits else spot
        return remote(source, spot, row_send.at[mask], row_recv.at[mask], at_level(low))

    def pair_copy(mask):
        spot = rows_scr.at[floor_of(mask), core]
        source = normed_ref if isinstance(mask, int) and mask == 0 else spot
        return remote(source, spot, pair_send.at[mask], pair_recv.at[mask], partner)

    def out_copy(mask, away):
        floor = floor_of(mask)
        return remote(
            stage.at[floor, column(away)], own_in.at[floor, here],
            out_send.at[mask, away], out_recv.at[mask, away], {"sp": column(away)},
        )

    def side_copy(mask, away):
        return remote(
            own_in.at[floor_of(mask), column(away)], other_in.at[mask % 2, column(away)],
            side_send.at[mask, away], side_recv.at[mask, away], partner,
        )

    def sum_copy(mask):
        return remote(
            other_out.at[mask % 2], other_got.at[mask % 2], sum_send.at[mask], sum_recv.at[mask],
            partner,
        )

    def back_copy(mask, away):
        floor = floor_of(mask)
        return remote(
            stage.at[floor, column(away)], returned.at[floor, here],
            back_send.at[mask, away], back_recv.at[mask, away], {"sp": column(away)},
        )

    def hand(mask):
        return remote(give.at[mask], take.at[mask], give_send.at[mask], take_recv.at[mask], partner)

    def post(mask):
        return remote(
            ship.at[mask], land.at[mask], ship_send.at[mask], land_recv.at[mask], at_level(mask)
        )

    rows_scr[level, core] = normed_ref[...]
    for bit in bits:
        row_copy(bit).start()

    def routes_of(mask):
        floor = floor_of(mask)
        return routes_ref[2 * floor] + routes_ref[2 * floor + 1]

    def dispatch(mask):
        floor = floor_of(mask)
        pair_copy(mask).start()
        tile = routes_of(mask)
        code = (
            lax.broadcasted_iota(jnp.int32, (slots, tokens), 0) + core * slots
        ).astype(jnp.float32)
        chosen = (tile[0:1, 0:tokens] == code) | (tile[1:2, 0:tokens] == code)
        chosen = jnp.where(chosen, 1.0, 0.0).astype(jnp.bfloat16)
        pair_copy(mask).wait_recv()
        width = min(512, features)
        for start in range(0, features, width):
            lanes = slice(start, start + width)
            rows = rows_scr[floor, :, :, lanes].reshape(tokens, width)
            picked = jnp.dot(chosen, rows, preferred_element_type=jnp.float32)
            stage[floor, :, :, lanes] = picked.astype(jnp.bfloat16).reshape(peers, share, width)
        own_in[floor, here] = stage[floor, here]
        for away in away_order:
            out_copy(mask, away).start()

    def arrive_and_dispatch(mask):
        row_copy(mask).wait_recv()
        for bit in bits[:-1]:

            @pl.when(mask % (2 * bit) == 0)
            def _():
                row_copy(mask + bit).start()

        dispatch(mask)

    dispatch(0)
    for mask in range(1, min(AHEAD, levels)):
        arrive_and_dispatch(mask)
    for load in loads:
        load.wait()

    def expert(index, source, store):
        hid = gate_w.shape[2]
        width = min(256, hid)

        def up_tile(n, _):
            lanes = pl.ds(pl.multiple_of(n * width, width), width)
            x = source[...].reshape(slots, features)
            gate = jnp.dot(x, gate_w[index, :, lanes], preferred_element_type=jnp.float32)
            up = jnp.dot(x, up_w[index, :, lanes], preferred_element_type=jnp.float32)
            hidden[:, lanes] = (silu(gate) * up).astype(jnp.bfloat16)
            return 0

        lax.fori_loop(0, hid // width, up_tile, 0)
        wide = min(512, features)

        def down_tile(n, _):
            lanes = pl.ds(pl.multiple_of(n * wide, wide), wide)
            store(
                lanes,
                jnp.dot(hidden[...], down_w[index, :, lanes], preferred_element_type=jnp.float32),
            )
            return 0

        lax.fori_loop(0, features // wide, down_tile, 0)

    def one_floor(mask, _):
        floor = floor_of(mask)
        side_copy(mask, 0).start()
        for away in away_order:
            out_copy(mask, away).wait_recv()
            side_copy(mask, away).start()
        if AHEAD < levels:

            @pl.when(mask + AHEAD < levels)
            def _():
                arrive_and_dispatch(mask + AHEAD)

        for away in range(peers):
            side_copy(mask, away).wait_recv()

        @pl.when(mask >= 2)
        def _():
            sum_copy(mask - 2).wait_send()

        def give_out(lanes, value):
            other_out[mask % 2, :, lanes] = value.astype(jnp.bfloat16)

        def keep(lanes, value):
            kept[:, lanes] = value

        expert(1 - core, other_in.at[mask % 2], give_out)
        sum_copy(mask).start()
        expert(core, own_in.at[floor], keep)
        for away in away_order:
            out_copy(mask, away).wait_send()
        sum_copy(mask).wait_recv()
        both = (kept[...] + other_got[mask % 2].astype(jnp.float32)).astype(jnp.bfloat16)
        stage[floor] = both.reshape(peers, share, features)
        returned[floor, here] = stage[floor, here]

        @pl.when(mask >= levels // 2)
        def _():
            for away in away_order:
                back_copy(mask, away).start()

        return 0

    lax.fori_loop(0, levels, one_floor, 0)
    for mask in range(levels // 2 - 1, -1, -1):
        for away in away_order:
            back_copy(mask, away).start()

    def turn_mask(turn):
        return jnp.where(turn < levels // 2, turn + levels // 2, levels - 1 - turn)

    def pass_on(mask):
        hand(mask).wait_recv()
        ship[mask] = (mine_scr[mask] + take[mask].astype(jnp.float32)).astype(jnp.bfloat16)
        post(mask).start()

    def combine(turn, _):
        mask = turn_mask(turn)
        tile = routes_of(mask)
        size = tile.shape[1]
        turned = jnp.transpose(
            jnp.concatenate([tile, jnp.zeros((size - tile.shape[0], size), jnp.float32)], axis=0)
        )[0:tokens, :]
        code = (
            lax.broadcasted_iota(jnp.int32, (tokens, slots), 1) + core * slots
        ).astype(jnp.float32)
        weight = jnp.where(turned[:, 0:1] == code, turned[:, 2:3], 0.0) + jnp.where(
            turned[:, 1:2] == code, turned[:, 3:4], 0.0
        )
        high = weight.astype(jnp.bfloat16)
        low = (weight - high.astype(jnp.float32)).astype(jnp.bfloat16)
        for away in away_order:
            back_copy(mask, away).wait_recv()
        width = min(512, features)
        for start in range(0, features, width):
            lanes = slice(start, start + width)
            got = returned[floor_of(mask), :, :, lanes].reshape(slots, width)
            full_scr[:, lanes] = jnp.dot(
                high, got, preferred_element_type=jnp.float32
            ) + jnp.dot(low, got, preferred_element_type=jnp.float32)
        own = pl.multiple_of(core * owned, owned)
        other = pl.multiple_of((1 - core) * owned, owned)
        give[mask] = full_scr[pl.ds(other, owned), :].astype(jnp.bfloat16)
        hand(mask).start()
        mine_scr[mask] = full_scr[pl.ds(own, owned), :]

        @pl.when(turn < levels - 1)
        def _():
            pass_on(mask)

        return 0

    settle()
    lax.fori_loop(0, levels, combine, 0)
    hand(0).wait_recv()
    total = mine_scr[0] + take[0].astype(jnp.float32)
    for mask in range(1, levels):
        post(mask).wait_recv()
        total = total + land[mask].astype(jnp.float32)
    out_ref[...] = after_ref[...].astype(jnp.float32) + total

    for mask in range(levels):
        pair_copy(mask).wait_send()
        hand(mask).wait_send()
        if mask:
            row_copy(mask).wait_send()
            post(mask).wait_send()
        if mask + 2 >= levels:
            sum_copy(mask).wait_send()
        for away in range(peers):
            side_copy(mask, away).wait_send()
            if away:
                back_copy(mask, away).wait_send()


def layer_kernel(experts_here, share, counts, *refs):
    refs = list(refs)

    def take(number):
        out = refs[:number]
        del refs[:number]
        return out

    near = take(counts[0])
    far = take(counts[1])
    (out_ref,) = take(1)
    loaded = take(counts[1])
    after_ref, normed_ref, routes = take(3)
    mixer_own = take(counts[2])
    shared = take(6)
    mixer_flags = take(10)
    experts_own = take(9)
    experts_flags = take(16)
    (load_sem,) = take(1)
    loads = [
        pltpu.make_async_copy(source, target, load_sem.at[index])
        for index, (source, target) in enumerate(zip(far, loaded))
    ]
    for load in loads:
        load.start()
    here, peers = lax.axis_index("sp"), lax.axis_size("sp")
    seat, seats = lax.axis_index("tp"), lax.axis_size("tp")
    greet(
        [{"sp": lax.rem(here + away, peers)} for away in range(1, peers)]
        + [{"tp": lax.rem(seat + away, seats)} for away in range(1, seats)]
    )
    for load in loads[0:3]:
        load.wait()
    settle = mixer_part(
        *loaded[0:3], *near, *loaded[3:6], loads[3:6], after_ref, normed_ref, routes, experts_here, share,
        *mixer_own, *shared, *mixer_flags,
    )
    experts_part(
        normed_ref, after_ref, routes, out_ref, loads[6:], settle,
        *experts_own, *shared, *loaded[6:], *experts_flags,
    )


def per_device(
    skip_stream_entry,
    result_switch_mapped,
    channel_feed_mapped,
    write_coefficient_mapped,
    emission_coefficient_mapped,
    channel_feed_taps,
    write_coefficient_taps,
    emission_coefficient_taps,
    raw_increments,
    channel_log_fade_speed,
    extra_log_fade,
    cluster_scaling_factor,
    blend_result_matrix,
    routing_scaling_factor,
    specialist_switch_matrix,
    specialist_widen_matrix,
    specialist_contract_matrix,
    picked_specialists,
    router_affinities,
):
    count, inner_here = channel_feed_mapped.shape
    owned, features = skip_stream_entry.shape
    experts_here, _, units = specialist_switch_matrix.shape
    peers, seats = lax.axis_size("sp"), lax.axis_size("tp")
    levels = seats // 2
    groups = write_coefficient_mapped.shape[1] // STATE
    width = inner_here // groups
    rows = 2 * (width // HEAD_DIM)
    blocks = count // BLOCK
    depth = STATE + 16
    capacity = max(2, 3 * TOP * owned // (2 * experts_here * peers))
    share = 2 * (-(-capacity // 8) * 8)
    slots = peers * share
    vmem, anywhere = pl.BlockSpec(memory_space=pltpu.VMEM), pl.BlockSpec(memory_space=pl.ANY)

    def half(*shape):
        return pltpu.VMEM(shape, jnp.bfloat16)

    def full(*shape):
        return pltpu.VMEM(shape, jnp.float32)

    def flags(*shape):
        return pltpu.SemaphoreType.DMA(shape)

    near = [
        channel_feed_taps, write_coefficient_taps, emission_coefficient_taps, raw_increments,
        channel_log_fade_speed, extra_log_fade, picked_specialists.T, router_affinities.T,
        cluster_scaling_factor.reshape(1, -1), routing_scaling_factor.reshape(1, -1),
    ]
    far = [
        channel_feed_mapped, write_coefficient_mapped, emission_coefficient_mapped,
        result_switch_mapped, skip_stream_entry, blend_result_matrix,
        specialist_switch_matrix, specialist_widen_matrix, specialist_contract_matrix,
    ]
    lines = groups * STATE
    mixer_own = [
        full(count + 2 * RIM, inner_here), full(count + 2 * RIM, lines), full(count + 2 * RIM, lines),
        half(EDGE, inner_here), half(EDGE, lines), half(EDGE, lines),
        half(EDGE, inner_here), half(EDGE, lines), half(EDGE, lines),
        full(groups, 2 * rows, count), full(count, inner_here), half(groups, blocks, STATE, BLOCK),
        half(count, lines), full(groups, blocks, rows, BLOCK), full(groups, blocks, BLOCK, rows),
        half(groups, blocks, STATE, 2 * width), half(2, groups, depth, width),
        half(peers, groups, depth, width), full(count, inner_here), full(groups, count, rows),
        half(groups, STATE, 2 * width), full(8, 128),
    ]
    slab = (levels, owned, features)
    shared = [full(2 * owned, features), full(*slab)] + [half(*slab)] * 4
    mixer_flags = [
        flags(2, 3), flags(2, 3), flags(groups, peers - 1), flags(groups, peers - 1),
        flags(seats - 1), flags(seats - 1), flags(levels), flags(levels), flags(levels), flags(levels),
    ]
    experts_own = [
        half(levels, 2, owned, features),
        half(levels, peers, share, features),
        half(levels, peers, share, features),
        half(2, peers, share, features),
        half(2, slots, features),
        half(2, slots, features),
        full(slots, features),
        half(slots, units),
        half(levels, peers, share, features),
    ]
    experts_flags = [
        flags(levels), flags(levels), flags(levels), flags(levels),
        flags(levels, peers), flags(levels, peers), flags(levels, peers), flags(levels, peers),
        flags(levels), flags(levels), flags(levels, peers), flags(levels, peers),
        flags(levels), flags(levels), flags(levels), flags(levels),
    ]
    return pl.pallas_call(
        functools.partial(layer_kernel, experts_here, share, (len(near), len(far), len(mixer_own))),
        in_specs=[vmem] * len(near) + [anywhere] * len(far),
        out_specs=vmem,
        out_shape=jax.ShapeDtypeStruct((owned, features), jnp.float32),
        scratch_shapes=[half(*array.shape) for array in far]
        + [half(owned, features), half(owned, features), full(seats, 8, 128)]
        + mixer_own + shared + mixer_flags + experts_own + experts_flags + [flags(len(far))],
        compiler_params=pltpu.CompilerParams(
            collective_id=0, has_side_effects=True, vmem_limit_bytes=67043328
        ),
        name="layer",
    )(*near, *far).astype(jnp.bfloat16)


def solution(mesh):
    in_specs = (
        P(("sp", "tp"), None),
        P("sp", "tp"),
        P("sp", "tp"),
        P("sp", "tp"),
        P("sp", "tp"),
        P(None, "tp"),
        P(None, "tp"),
        P(None, "tp"),
        P(None, "tp", "sp"),
        P(None, "tp"),
        P(None, "tp", "sp"),
        P("tp"),
        P("tp", None),
        P(),
        P("sp", None, "tp"),
        P("sp", None, "tp"),
        P("sp", "tp", None),
        P(("sp", "tp"), None),
        P(("sp", "tp"), None),
    )
    out_specs = P(("sp", "tp"), None)
    return jax.shard_map(
        per_device, mesh=mesh, in_specs=in_specs, out_specs=out_specs, check_vma=False
    )
```

```python
import functools

import jax
import jax.numpy as jnp
from jax import lax
from jax.experimental import pallas as pl
from jax.experimental.pallas import tpu as pltpu
from jax.sharding import PartitionSpec as P

WIDTH = 2048
HEAD_DIM = 64
GROUPS = 16
STATE = 128
CONV_W = 5
BLOCK = 128
TOP = 2
INNER = 4096


EPSILON = 1e-06
HIGHEST_MODE = lax.Precision.HIGHEST


MESH_IDS = pl.DeviceIdType.MESH
RIM = 8
EDGE = 16


def spread_heads(columns, per_group):
    rows = columns.shape[0]
    lane = lax.broadcasted_iota(jnp.int32, (rows, per_group * HEAD_DIM), 1) // HEAD_DIM
    out = jnp.broadcast_to(columns[:, 0:1], lane.shape)
    for head in range(1, per_group):
        out = jnp.where(lane == head, jnp.broadcast_to(columns[:, head : head + 1], lane.shape), out)
    return out


def silu(value):
    return value * jax.nn.sigmoid(value)


def conv_block(scratch, taps, block, lanes):
    rim = taps.shape[0] // 2
    total = None
    for offset in range(taps.shape[0]):
        start = RIM - rim + offset + block * BLOCK
        term = taps[offset : offset + 1, lanes].astype(jnp.float32) * scratch[start : start + BLOCK, lanes]
        total = term if total is None else total + term
    return silu(total)


def flip(index, mask, count):
    out, bit = index, 1
    while bit < count:
        out = out + ((mask // bit) % 2) * (1 - 2 * ((index // bit) % 2)) * bit
        bit = 2 * bit
    return out


def low_bit(mask, count):
    out, bit = 0, count // 2
    while bit >= 1:
        odd = (mask // bit) % 2
        out = odd * bit + (1 - odd) * out
        bit = bit // 2
    return out


def remote(source, target, send_sem, recv_sem, where):
    return pltpu.make_async_remote_copy(
        src_ref=source, dst_ref=target, send_sem=send_sem, recv_sem=recv_sem,
        device_id=where, device_id_type=MESH_IDS,
    )


def greet(places):
    barrier = pltpu.get_barrier_semaphore()
    for place in places:
        pl.semaphore_signal(barrier, inc=1, device_id=place, device_id_type=MESH_IDS)
    pl.semaphore_wait(barrier, len(places))


def write_route(picks_ref, affinity_ref, route_scr, experts_here, share):
    owned = picks_ref.shape[1]
    peers, core = lax.axis_size("sp"), lax.axis_index("tp") % 2
    picks, affinity = picks_ref[...], affinity_ref[...]
    count = -(-experts_here * peers // 8) * 8
    expert = lax.broadcasted_iota(jnp.int32, (count, owned), 0)
    marks = [jnp.where(picks[k : k + 1, :] == expert, 1.0, 0.0) for k in range(TOP)]
    earlier = jnp.where(
        lax.broadcasted_iota(jnp.int32, (owned, owned), 0)
        < lax.broadcasted_iota(jnp.int32, (owned, owned), 1),
        1.0,
        0.0,
    ).astype(jnp.bfloat16)
    ahead = jnp.dot(
        (marks[0] + marks[1]).astype(jnp.bfloat16), earlier, preferred_element_type=jnp.float32
    )
    base = (expert % experts_here) * (peers * share) + (expert // experts_here) * share
    base = (base + core * (share // 2)).astype(jnp.float32) + ahead
    places = [jnp.sum(mark * base, axis=0, keepdims=True) for mark in marks]
    whole = affinity[0:1, :] + affinity[1:2, :]
    lines = jnp.concatenate(
        places
        + [affinity[0:1, :] / whole, affinity[1:2, :] / whole]
        + [jnp.zeros((8 - 2 * TOP, owned), jnp.float32)],
        axis=0,
    )
    blank = jnp.zeros_like(lines)
    rest = [] if 2 * owned == 128 else [jnp.zeros((8, 128 - 2 * owned), jnp.float32)]
    route_scr[...] = jnp.concatenate(
        [jnp.where(core == 0, lines, blank), jnp.where(core == 0, blank, lines)] + rest, axis=1
    )


def mixer_part(
    x_ref, b_ref, c_ref, x_taps, b_taps, c_taps, inc_ref, speed_ref, extra_ref, picks_ref,
    affinity_ref, gain_ref, norm_gain_ref, gate_ref, skip_ref, weight_ref, loads, after_ref,
    normed_ref, routes, experts_here, share,
    x_pad, b_pad, c_pad, x_low, b_low, c_low, x_high, b_high, c_high, fade_scr, x_kept, b_kept,
    c_kept, cum_scr, col_scr, entry_scr, state_ref, target, y_ref, reach_ref, carry_scr, route_scr,
    full_scr, mine_scr, give, take, ship, land,
    edge_send, edge_recv, state_send, state_recv, route_send, route_recv,
    give_send, take_recv, ship_send, land_recv,
):
    count, inner_here = x_ref.shape
    groups = b_ref.shape[1] // STATE
    width = inner_here // groups
    per_group = width // HEAD_DIM
    rows = 2 * per_group
    blocks = count // BLOCK
    rim = x_taps.shape[0] // 2
    here, peers = lax.axis_index("sp"), lax.axis_size("sp")
    seat, seats = lax.axis_index("tp"), lax.axis_size("tp")
    levels = seats // 2
    core, level = seat % 2, seat // 2
    owned, features = skip_ref.shape
    partner = {"tp": seat + 1 - 2 * core}

    edges = []
    for index, (source, low, high) in enumerate(
        ((x_ref, x_low, x_high), (b_ref, b_low, b_high), (c_ref, c_low, c_high))
    ):
        onward = remote(
            source.at[pl.ds(count - EDGE, EDGE)], low, edge_send.at[0, index],
            edge_recv.at[0, index], {"sp": lax.rem(here + 1, peers)},
        )
        back = remote(
            source.at[pl.ds(0, EDGE)], high, edge_send.at[1, index],
            edge_recv.at[1, index], {"sp": lax.rem(here + peers - 1, peers)},
        )
        edges.append((onward, back))

    @pl.when(here < peers - 1)
    def _():
        for onward, _ in edges:
            onward.start()

    @pl.when(here > 0)
    def _():
        for _, back in edges:
            back.start()

    write_route(picks_ref, affinity_ref, route_scr, experts_here, share)
    route_copies = [
        remote(
            route_scr, routes.at[seat], route_send.at[away - 1], route_recv.at[away - 1],
            {"tp": lax.rem(seat + away, seats)},
        )
        for away in range(1, seats)
    ]
    for copy in route_copies:
        copy.start()
    routes[seat] = route_scr[...]
    target[here] = jnp.zeros(target.shape[1:], target.dtype)

    heads = inc_ref.shape[1]
    square_at = [lax.broadcasted_iota(jnp.int32, (heads, heads), axis) for axis in range(2)]
    for first in range(2):
        raw = inc_ref[first].astype(jnp.float32)
        step = jnp.maximum(raw, 0.0) + jnp.log1p(jnp.exp(-jnp.abs(raw)))
        line = jnp.broadcast_to(speed_ref[first : first + 1, :], (heads, heads))
        speed = jnp.sum(
            jnp.where(square_at[0] == square_at[1], jnp.exp(line), 0.0), axis=1, keepdims=True
        )
        fade = -step * speed + extra_ref[first]
        for group in range(groups):
            mine = slice(group * per_group, (group + 1) * per_group)
            spot = first * per_group
            fade_scr[group, spot : spot + per_group, :] = fade[mine, :]
            fade_scr[group, rows + spot : rows + spot + per_group, :] = step[mine, :]
    i_at = lax.broadcasted_iota(jnp.int32, (BLOCK, BLOCK), 0)
    j_at = lax.broadcasted_iota(jnp.int32, (BLOCK, BLOCK), 1)
    up_to = (i_at <= j_at).astype(jnp.float32)
    from_on = (i_at >= j_at).astype(jnp.float32)
    col_at = lax.broadcasted_iota(jnp.int32, (1, rows), 1)
    half_lane = lax.broadcasted_iota(jnp.int32, (BLOCK, 2 * HEAD_DIM), 1) < HEAD_DIM

    spots = [(group, block) for group in range(groups) for block in range(blocks)]
    fades = jnp.concatenate(
        [fade_scr[g, 0:rows, b * BLOCK : (b + 1) * BLOCK] for g, b in spots], axis=0
    )
    onward = jnp.dot(fades, up_to, precision=HIGHEST_MODE, preferred_element_type=jnp.float32)
    back = jnp.dot(fades, from_on, precision=HIGHEST_MODE, preferred_element_type=jnp.float32)
    row_at = lax.broadcasted_iota(jnp.int32, fades.shape, 0)
    sums = jnp.where(row_at % rows < per_group, onward, back)
    lines, columns, per_turn = [], {}, BLOCK // (2 * rows)
    for index, (g, b) in enumerate(spots):
        cum = sums[index * rows : (index + 1) * rows, :]
        cum_scr[g, b] = cum
        lines += [cum, fade_scr[g, rows : 2 * rows, b * BLOCK : (b + 1) * BLOCK]]
    for start in range(0, len(spots), per_turn):
        part = lines[2 * start : 2 * (start + per_turn)]
        rest = BLOCK - rows * len(part)
        if rest:
            part = part + [jnp.zeros((rest, BLOCK), jnp.float32)]
        turned = jnp.transpose(jnp.concatenate(part, axis=0))
        for offset, spot in enumerate(spots[start : start + per_turn]):
            lane = 2 * rows * offset
            columns[spot] = (
                turned[:, lane : lane + rows], turned[:, lane + rows : lane + 2 * rows]
            )

    for pad, source in ((x_pad, x_ref), (b_pad, b_ref), (c_pad, c_ref)):
        pad[RIM : RIM + count, :] = source[...].astype(jnp.float32)

    @pl.when(here > 0)
    def _():
        for onward, _ in edges:
            onward.wait_recv()
        for pad, low in ((x_pad, x_low), (b_pad, b_low), (c_pad, c_low)):
            pad[RIM - rim : RIM, :] = low[...].astype(jnp.float32)[EDGE - rim : EDGE, :]

    @pl.when(here == 0)
    def _():
        for pad in (x_pad, b_pad, c_pad):
            pad[RIM - rim : RIM, :] = jnp.zeros((rim, pad.shape[1]), jnp.float32)

    @pl.when(here < peers - 1)
    def _():
        for _, back in edges:
            back.wait_recv()
        for pad, high in ((x_pad, x_high), (b_pad, b_high), (c_pad, c_high)):
            pad[RIM + count : RIM + count + rim, :] = high[...].astype(jnp.float32)[0:rim, :]

    @pl.when(here == peers - 1)
    def _():
        for pad in (x_pad, b_pad, c_pad):
            pad[RIM + count : RIM + count + rim, :] = jnp.zeros((rim, pad.shape[1]), jnp.float32)

    def state_copy(group, away):
        peer = flip(here, peers - away, peers)
        return remote(
            state_ref.at[jnp.where(peer > here, 0, 1), group], target.at[here, group],
            state_send.at[group, away - 1], state_recv.at[group, away - 1], {"sp": peer},
        )

    all_totals = []
    for group in range(groups):
        lanes_x = slice(group * width, (group + 1) * width)
        lanes_s = slice(group * STATE, (group + 1) * STATE)
        totals, parts = [], []
        for block in range(blocks):
            at = slice(block * BLOCK, (block + 1) * BLOCK)
            cum_col, step_col = columns[group, block]
            total = jnp.where(col_at < per_group, cum_col[BLOCK - 1 : BLOCK, :], cum_col[0:1, :])
            to_end = jnp.exp(total - cum_col) * step_col
            col_scr[group, block] = cum_col
            x = conv_block(x_pad, x_taps, block, lanes_x)
            b = conv_block(b_pad, b_taps, block, lanes_s)
            x_kept[at, lanes_x] = x
            b_turned = jnp.transpose(b).astype(jnp.bfloat16)
            b_kept[group, block] = b_turned
            weighted = jnp.concatenate(
                [
                    x * spread_heads(to_end[:, 0:per_group], per_group),
                    x * spread_heads(to_end[:, per_group:rows], per_group),
                ],
                axis=1,
            ).astype(jnp.bfloat16)
            parts.append(jnp.dot(b_turned, weighted, preferred_element_type=jnp.float32))
            totals.append(total)
        for first, order in ((0, range(blocks)), (1, range(blocks - 1, -1, -1))):
            lanes = slice(first * width, (first + 1) * width)
            held = jnp.zeros((STATE, width), jnp.float32)
            for block in order:
                entry_scr[group, block, :, lanes] = held.astype(jnp.bfloat16)
                factor = spread_heads(
                    jnp.exp(totals[block][:, first * per_group : (first + 1) * per_group]), per_group
                )
                held = held * factor + parts[block][:, lanes]
            state_ref[first, group, 0:STATE, :] = held.astype(jnp.bfloat16)
            whole = totals[0]
            for block in range(1, blocks):
                whole = whole + totals[block]
            whole = spread_heads(
                jnp.exp(whole[:, first * per_group : (first + 1) * per_group]), per_group
            )
            state_ref[first, group, STATE:, :] = jnp.broadcast_to(
                whole, (state_ref.shape[2] - STATE, width)
            ).astype(jnp.bfloat16)
        for away in range(1, peers):
            state_copy(group, away).start()
        all_totals.append(totals)

    for group in range(groups):
        lanes_s = slice(group * STATE, (group + 1) * STATE)
        totals = all_totals[group]
        for block in range(blocks):
            at = slice(block * BLOCK, (block + 1) * BLOCK)
            c_kept[at, lanes_s] = conv_block(c_pad, c_taps, block, lanes_s).astype(jnp.bfloat16)
            offset = jnp.zeros((1, rows), jnp.float32)
            for earlier in range(blocks):
                if earlier < block:
                    offset = offset + jnp.where(col_at < per_group, totals[earlier], 0.0)
                if earlier > block:
                    offset = offset + jnp.where(col_at < per_group, 0.0, totals[earlier])
            reach_ref[group, at, :] = jnp.exp(col_scr[group, block] + offset)

    def within(block):
        at = pl.ds(pl.multiple_of(block * BLOCK, BLOCK), BLOCK)
        for group in range(groups):
            lanes_x = slice(group * width, (group + 1) * width)
            lanes_s = slice(group * STATE, (group + 1) * STATE)
            step = fade_scr[group, rows : 2 * rows, at]
            cum, cum_col = cum_scr[group, block], col_scr[group, block]
            x = x_kept[at, lanes_x]
            c = c_kept[at, lanes_s]
            inner = jnp.dot(c, b_kept[group, block], preferred_element_type=jnp.float32)
            mixing = []
            for head in range(per_group):
                other = per_group + head
                gap = jnp.where(
                    i_at >= j_at,
                    cum_col[:, head : head + 1] - cum[head : head + 1, :],
                    cum_col[:, other : other + 1] - cum[other : other + 1, :],
                )
                own, opposite = step[head : head + 1, :], step[other : other + 1, :]
                amount = jnp.where(
                    i_at > j_at, own, jnp.where(i_at < j_at, opposite, own + opposite)
                )
                mixing.append((jnp.exp(gap) * amount * inner).astype(jnp.bfloat16))
            pieces = []
            for pair in range(per_group // 2):
                x_pair = x[:, pair * 2 * HEAD_DIM : (pair + 1) * 2 * HEAD_DIM]
                both = jnp.concatenate(
                    [jnp.where(half_lane, x_pair, 0.0), jnp.where(half_lane, 0.0, x_pair)], axis=0
                ).astype(jnp.bfloat16)
                left = jnp.concatenate([mixing[2 * pair], mixing[2 * pair + 1]], axis=1)
                pieces.append(jnp.dot(left, both, preferred_element_type=jnp.float32))
            readout = jnp.dot(c, entry_scr[group, block], preferred_element_type=jnp.float32)
            fade_in = jnp.exp(cum_col)
            y_ref[at, lanes_x] = (
                jnp.concatenate(pieces, axis=1)
                + readout[:, :width] * spread_heads(fade_in[:, 0:per_group], per_group)
                + readout[:, width:] * spread_heads(fade_in[:, per_group:rows], per_group)
            )

    def at_level(mask):
        return {"tp": 2 * flip(level, mask, levels) + core}

    def hand(mask):
        return remote(give.at[mask], take.at[mask], give_send.at[mask], take_recv.at[mask], partner)

    def post(mask):
        return remote(
            ship.at[mask], land.at[mask], ship_send.at[mask], land_recv.at[mask],
            at_level(low_bit(mask, levels)),
        )

    def block_mask(turn):
        return jnp.where(turn < levels // 2, levels - 1 - 2 * turn, 2 * levels - 2 - 2 * turn)

    woven = 2 * owned == BLOCK and blocks == levels
    early = min(2, levels) if woven else blocks

    def first_blocks(turn, _):
        within(flip(level, block_mask(turn), levels) if woven else turn)
        return 0

    lax.fori_loop(0, early, first_blocks, 0)
    for load in loads:
        load.wait()
    for group in range(groups):
        for away in range(1, peers):
            state_copy(group, away).wait_recv()
        for first in range(2):
            held = jnp.zeros((STATE, width), jnp.float32)
            order = range(peers) if first == 0 else range(peers - 1, -1, -1)
            for peer in order:
                fresh = target[peer, group, 0:STATE, :].astype(jnp.float32)
                factor = target[peer, group, STATE : STATE + 1, :].astype(jnp.float32)
                reached = peer < here if first == 0 else peer > here
                held = jnp.where(reached, held * factor + fresh, held)
            carry_scr[group, :, first * width : (first + 1) * width] = held.astype(jnp.bfloat16)

    def gather(mask, lows):
        hand(mask).wait_recv()
        total = mine_scr[mask] + take[mask].astype(jnp.float32)
        for low in lows:
            post(mask + low).wait_recv()
            total = total + land[mask + low].astype(jnp.float32)
        return total

    def pass_on(mask, lows):
        ship[mask] = gather(mask, lows).astype(jnp.bfloat16)
        post(mask).start()

    def one_block(turn, _):
        mask = block_mask(turn)
        at = pl.ds(pl.multiple_of(flip(level, mask, levels) * (2 * owned), 2 * owned), 2 * owned)
        mixed = []
        for group in range(groups):
            lanes = slice(group * width, (group + 1) * width)
            c = c_kept[at, group * STATE : (group + 1) * STATE]
            readout = jnp.dot(c, carry_scr[group], preferred_element_type=jnp.float32)
            reach = reach_ref[group, at, :]
            y = (
                y_ref[at, lanes]
                + readout[:, :width] * spread_heads(reach[:, 0:per_group], per_group)
                + readout[:, width:] * spread_heads(reach[:, per_group:rows], per_group)
            )
            gated = y * silu(gate_ref[at, lanes].astype(jnp.float32))
            square = jnp.mean(gated * gated, axis=-1, keepdims=True)
            mixed.append(
                (gated * lax.rsqrt(square + EPSILON) * gain_ref[:, lanes]).astype(jnp.bfloat16)
            )
        rows_mixed = mixed[0] if groups == 1 else jnp.concatenate(mixed, axis=1)
        tile = min(512, features)
        for start in range(0, features, tile):
            full_scr[:, start : start + tile] = jnp.dot(
                rows_mixed, weight_ref[:, start : start + tile], preferred_element_type=jnp.float32
            )
        own = pl.multiple_of(core * owned, owned)
        other = pl.multiple_of((1 - core) * owned, owned)
        give[mask] = full_scr[pl.ds(other, owned), :].astype(jnp.bfloat16)
        hand(mask).start()
        mine_scr[mask] = full_scr[pl.ds(own, owned), :]

        if woven:

            @pl.when(turn + early < levels)
            def _():
                within(flip(level, block_mask(turn + early), levels))

        @pl.when(turn < levels // 2)
        def _():
            pass_on(mask, [])

        return 0

    lax.fori_loop(0, levels, one_block, 0)
    bits = [1 << n for n in range(levels.bit_length() - 1)]
    for bit in bits[1:]:
        for mask in range(levels - bit, 0, -2 * bit):
            pass_on(mask, [low for low in bits if low < bit])
    total = gather(0, bits)
    after = (skip_ref[...].astype(jnp.float32) + total).astype(jnp.bfloat16)
    after_ref[...] = after
    values = after.astype(jnp.float32)
    scale = lax.rsqrt(jnp.mean(values * values, axis=-1, keepdims=True) + EPSILON)
    normed_ref[...] = (values * scale * norm_gain_ref[...]).astype(jnp.bfloat16)
    for copy in route_copies:
        copy.wait_recv()

    def settle():
        for mask in range(levels):
            hand(mask).wait_send()
            if mask:
                post(mask).wait_send()
        for copy in route_copies:
            copy.wait_send()
        for group in range(groups):
            for away in range(1, peers):
                state_copy(group, away).wait_send()

        @pl.when(here < peers - 1)
        def _():
            for onward, _ in edges:
                onward.wait_send()

        @pl.when(here > 0)
        def _():
            for _, back in edges:
                back.wait_send()

    return settle


AHEAD = 2


def experts_part(
    normed_ref, after_ref, routes_ref, out_ref, loads, settle,
    rows_scr, stage, own_in, other_in, other_out, other_got, kept, hidden, returned,
    full_scr, mine_scr, give, take, ship, land, gate_w, up_w, down_w,
    row_send, row_recv, pair_send, pair_recv, out_send, out_recv, side_send, side_recv,
    sum_send, sum_recv, back_send, back_recv, give_send, take_recv, ship_send, land_recv,
):
    here, peers = lax.axis_index("sp"), lax.axis_size("sp")
    seat = lax.axis_index("tp")
    levels = lax.axis_size("tp") // 2
    core, level = seat % 2, seat // 2
    owned, features = normed_ref.shape
    share = stage.shape[2]
    slots = peers * share
    tokens = 2 * owned
    partner = {"tp": seat + 1 - 2 * core}
    away_order = list(range(peers - 1, 0, -1))

    def floor_of(mask):
        return flip(level, mask, levels)

    def at_level(mask):
        return {"tp": 2 * floor_of(mask) + core}

    def column(away):
        return flip(here, away, peers)

    bits = [1 << n for n in range(levels.bit_length() - 1)]

    def row_copy(mask):
        low = low_bit(mask, levels)
        spot = rows_scr.at[floor_of(mask - low), core]
        source = normed_ref if isinstance(mask, int) and mask in bits else spot
        return remote(source, spot, row_send.at[mask], row_recv.at[mask], at_level(low))

    def pair_copy(mask):
        spot = rows_scr.at[floor_of(mask), core]
        source = normed_ref if isinstance(mask, int) and mask == 0 else spot
        return remote(source, spot, pair_send.at[mask], pair_recv.at[mask], partner)

    def out_copy(mask, away):
        floor = floor_of(mask)
        return remote(
            stage.at[floor, column(away)], own_in.at[floor, here],
            out_send.at[mask, away], out_recv.at[mask, away], {"sp": column(away)},
        )

    def side_copy(mask, away):
        return remote(
            own_in.at[floor_of(mask), column(away)], other_in.at[mask % 2, column(away)],
            side_send.at[mask, away], side_recv.at[mask, away], partner,
        )

    def sum_copy(mask):
        return remote(
            other_out.at[mask % 2], other_got.at[mask % 2], sum_send.at[mask], sum_recv.at[mask],
            partner,
        )

    def back_copy(mask, away):
        floor = floor_of(mask)
        return remote(
            stage.at[floor, column(away)], returned.at[floor, here],
            back_send.at[mask, away], back_recv.at[mask, away], {"sp": column(away)},
        )

    def hand(mask):
        return remote(give.at[mask], take.at[mask], give_send.at[mask], take_recv.at[mask], partner)

    def post(mask):
        return remote(
            ship.at[mask], land.at[mask], ship_send.at[mask], land_recv.at[mask], at_level(mask)
        )

    rows_scr[level, core] = normed_ref[...]
    for bit in bits:
        row_copy(bit).start()

    def routes_of(mask):
        floor = floor_of(mask)
        return routes_ref[2 * floor] + routes_ref[2 * floor + 1]

    def dispatch(mask):
        floor = floor_of(mask)
        pair_copy(mask).start()
        tile = routes_of(mask)
        code = (
            lax.broadcasted_iota(jnp.int32, (slots, tokens), 0) + core * slots
        ).astype(jnp.float32)
        chosen = (tile[0:1, 0:tokens] == code) | (tile[1:2, 0:tokens] == code)
        chosen = jnp.where(chosen, 1.0, 0.0).astype(jnp.bfloat16)
        pair_copy(mask).wait_recv()
        width = min(512, features)
        for start in range(0, features, width):
            lanes = slice(start, start + width)
            rows = rows_scr[floor, :, :, lanes].reshape(tokens, width)
            picked = jnp.dot(chosen, rows, preferred_element_type=jnp.float32)
            stage[floor, :, :, lanes] = picked.astype(jnp.bfloat16).reshape(peers, share, width)
        own_in[floor, here] = stage[floor, here]
        for away in away_order:
            out_copy(mask, away).start()

    def arrive_and_dispatch(mask):
        row_copy(mask).wait_recv()
        for bit in bits[:-1]:

            @pl.when(mask % (2 * bit) == 0)
            def _():
                row_copy(mask + bit).start()

        dispatch(mask)

    dispatch(0)
    for mask in range(1, min(AHEAD, levels)):
        arrive_and_dispatch(mask)
    for load in loads:
        load.wait()

    def expert(index, source, store):
        hid = gate_w.shape[2]
        width = min(256, hid)

        def up_tile(n, _):
            lanes = pl.ds(pl.multiple_of(n * width, width), width)
            x = source[...].reshape(slots, features)
            gate = jnp.dot(x, gate_w[index, :, lanes], preferred_element_type=jnp.float32)
            up = jnp.dot(x, up_w[index, :, lanes], preferred_element_type=jnp.float32)
            hidden[:, lanes] = (silu(gate) * up).astype(jnp.bfloat16)
            return 0

        lax.fori_loop(0, hid // width, up_tile, 0)
        wide = min(512, features)

        def down_tile(n, _):
            lanes = pl.ds(pl.multiple_of(n * wide, wide), wide)
            store(
                lanes,
                jnp.dot(hidden[...], down_w[index, :, lanes], preferred_element_type=jnp.float32),
            )
            return 0

        lax.fori_loop(0, features // wide, down_tile, 0)

    def one_floor(mask, _):
        floor = floor_of(mask)
        side_copy(mask, 0).start()
        for away in away_order:
            out_copy(mask, away).wait_recv()
            side_copy(mask, away).start()
        if AHEAD < levels:

            @pl.when(mask + AHEAD < levels)
            def _():
                arrive_and_dispatch(mask + AHEAD)

        for away in range(peers):
            side_copy(mask, away).wait_recv()

        @pl.when(mask >= 2)
        def _():
            sum_copy(mask - 2).wait_send()

        def give_out(lanes, value):
            other_out[mask % 2, :, lanes] = value.astype(jnp.bfloat16)

        def keep(lanes, value):
            kept[:, lanes] = value

        expert(1 - core, other_in.at[mask % 2], give_out)
        sum_copy(mask).start()
        expert(core, own_in.at[floor], keep)
        for away in away_order:
            out_copy(mask, away).wait_send()
        sum_copy(mask).wait_recv()
        both = (kept[...] + other_got[mask % 2].astype(jnp.float32)).astype(jnp.bfloat16)
        stage[floor] = both.reshape(peers, share, features)
        returned[floor, here] = stage[floor, here]

        @pl.when(mask >= levels // 2)
        def _():
            for away in away_order:
                back_copy(mask, away).start()

        return 0

    lax.fori_loop(0, levels, one_floor, 0)
    for mask in range(levels // 2 - 1, -1, -1):
        for away in away_order:
            back_copy(mask, away).start()

    def turn_mask(turn):
        return jnp.where(turn < levels // 2, turn + levels // 2, levels - 1 - turn)

    def pass_on(mask):
        hand(mask).wait_recv()
        ship[mask] = (mine_scr[mask] + take[mask].astype(jnp.float32)).astype(jnp.bfloat16)
        post(mask).start()

    def combine(turn, _):
        mask = turn_mask(turn)
        tile = routes_of(mask)
        size = tile.shape[1]
        turned = jnp.transpose(
            jnp.concatenate([tile, jnp.zeros((size - tile.shape[0], size), jnp.float32)], axis=0)
        )[0:tokens, :]
        code = (
            lax.broadcasted_iota(jnp.int32, (tokens, slots), 1) + core * slots
        ).astype(jnp.float32)
        weight = jnp.where(turned[:, 0:1] == code, turned[:, 2:3], 0.0) + jnp.where(
            turned[:, 1:2] == code, turned[:, 3:4], 0.0
        )
        high = weight.astype(jnp.bfloat16)
        low = (weight - high.astype(jnp.float32)).astype(jnp.bfloat16)
        for away in away_order:
            back_copy(mask, away).wait_recv()
        first_high, second_high = high[0:owned, :], high[owned:, :]
        first_low, second_low = low[0:owned, :], low[owned:, :]

        def product(pick):
            top = jnp.where(pick == 0, first_high, second_high)
            rest = jnp.where(pick == 0, first_low, second_low)
            got = returned[floor_of(mask)].reshape(slots, features)
            return jnp.dot(top, got, preferred_element_type=jnp.float32) + jnp.dot(
                rest, got, preferred_element_type=jnp.float32
            )

        give[mask] = product(1 - core).astype(jnp.bfloat16)
        hand(mask).start()
        mine_scr[mask] = product(core)

        @pl.when(turn < levels - 1)
        def _():
            pass_on(mask)

        return 0

    settle()
    lax.fori_loop(0, levels, combine, 0)
    hand(0).wait_recv()
    total = mine_scr[0] + take[0].astype(jnp.float32)
    for mask in range(1, levels):
        post(mask).wait_recv()
        total = total + land[mask].astype(jnp.float32)
    out_ref[...] = after_ref[...].astype(jnp.float32) + total

    for mask in range(levels):
        pair_copy(mask).wait_send()
        hand(mask).wait_send()
        if mask:
            row_copy(mask).wait_send()
            post(mask).wait_send()
        if mask + 2 >= levels:
            sum_copy(mask).wait_send()
        for away in range(peers):
            side_copy(mask, away).wait_send()
            if away:
                back_copy(mask, away).wait_send()


def layer_kernel(experts_here, share, counts, *refs):
    refs = list(refs)

    def take(number):
        out = refs[:number]
        del refs[:number]
        return out

    near = take(counts[0])
    far = take(counts[1])
    (out_ref,) = take(1)
    loaded = take(counts[1])
    after_ref, normed_ref, routes = take(3)
    mixer_own = take(counts[2])
    shared = take(6)
    mixer_flags = take(10)
    experts_own = take(9)
    experts_flags = take(16)
    (load_sem,) = take(1)
    loads = [
        pltpu.make_async_copy(source, target, load_sem.at[index])
        for index, (source, target) in enumerate(zip(far, loaded))
    ]
    for load in loads[0:3]:
        load.start()
    here, peers = lax.axis_index("sp"), lax.axis_size("sp")
    seat, seats = lax.axis_index("tp"), lax.axis_size("tp")
    greet(
        [{"sp": lax.rem(here + away, peers)} for away in range(1, peers)]
        + [{"tp": lax.rem(seat + away, seats)} for away in range(1, seats)]
    )
    for load in loads[0:3]:
        load.wait()
    for load in loads[3:]:
        load.start()
    settle = mixer_part(
        *loaded[0:3], *near, *loaded[3:6], loads[3:6], after_ref, normed_ref, routes, experts_here, share,
        *mixer_own, *shared, *mixer_flags,
    )
    experts_part(
        normed_ref, after_ref, routes, out_ref, loads[6:], settle,
        *experts_own, *shared, *loaded[6:], *experts_flags,
    )


def per_device(
    skip_stream_entry,
    result_switch_mapped,
    channel_feed_mapped,
    write_coefficient_mapped,
    emission_coefficient_mapped,
    channel_feed_taps,
    write_coefficient_taps,
    emission_coefficient_taps,
    raw_increments,
    channel_log_fade_speed,
    extra_log_fade,
    cluster_scaling_factor,
    blend_result_matrix,
    routing_scaling_factor,
    specialist_switch_matrix,
    specialist_widen_matrix,
    specialist_contract_matrix,
    picked_specialists,
    router_affinities,
):
    count, inner_here = channel_feed_mapped.shape
    owned, features = skip_stream_entry.shape
    experts_here, _, units = specialist_switch_matrix.shape
    peers, seats = lax.axis_size("sp"), lax.axis_size("tp")
    levels = seats // 2
    groups = write_coefficient_mapped.shape[1] // STATE
    width = inner_here // groups
    rows = 2 * (width // HEAD_DIM)
    blocks = count // BLOCK
    depth = STATE + 16
    capacity = max(2, 3 * TOP * owned // (2 * experts_here * peers))
    share = 2 * (-(-capacity // 8) * 8)
    slots = peers * share
    vmem, anywhere = pl.BlockSpec(memory_space=pltpu.VMEM), pl.BlockSpec(memory_space=pl.ANY)

    def half(*shape):
        return pltpu.VMEM(shape, jnp.bfloat16)

    def full(*shape):
        return pltpu.VMEM(shape, jnp.float32)

    def flags(*shape):
        return pltpu.SemaphoreType.DMA(shape)

    near = [
        channel_feed_taps, write_coefficient_taps, emission_coefficient_taps, raw_increments,
        channel_log_fade_speed, extra_log_fade, picked_specialists.T, router_affinities.T,
        cluster_scaling_factor.reshape(1, -1), routing_scaling_factor.reshape(1, -1),
    ]
    far = [
        channel_feed_mapped, write_coefficient_mapped, emission_coefficient_mapped,
        result_switch_mapped, skip_stream_entry, blend_result_matrix,
        specialist_switch_matrix, specialist_widen_matrix, specialist_contract_matrix,
    ]
    lines = groups * STATE
    mixer_own = [
        full(count + 2 * RIM, inner_here), full(count + 2 * RIM, lines), full(count + 2 * RIM, lines),
        half(EDGE, inner_here), half(EDGE, lines), half(EDGE, lines),
        half(EDGE, inner_here), half(EDGE, lines), half(EDGE, lines),
        full(groups, 2 * rows, count), full(count, inner_here), half(groups, blocks, STATE, BLOCK),
        half(count, lines), full(groups, blocks, rows, BLOCK), full(groups, blocks, BLOCK, rows),
        half(groups, blocks, STATE, 2 * width), half(2, groups, depth, width),
        half(peers, groups, depth, width), full(count, inner_here), full(groups, count, rows),
        half(groups, STATE, 2 * width), full(8, 128),
    ]
    slab = (levels, owned, features)
    shared = [full(2 * owned, features), full(*slab)] + [half(*slab)] * 4
    mixer_flags = [
        flags(2, 3), flags(2, 3), flags(groups, peers - 1), flags(groups, peers - 1),
        flags(seats - 1), flags(seats - 1), flags(levels), flags(levels), flags(levels), flags(levels),
    ]
    experts_own = [
        half(levels, 2, owned, features),
        half(levels, peers, share, features),
        half(levels, peers, share, features),
        half(2, peers, share, features),
        half(2, slots, features),
        half(2, slots, features),
        full(slots, features),
        half(slots, units),
        half(levels, peers, share, features),
    ]
    experts_flags = [
        flags(levels), flags(levels), flags(levels), flags(levels),
        flags(levels, peers), flags(levels, peers), flags(levels, peers), flags(levels, peers),
        flags(levels), flags(levels), flags(levels, peers), flags(levels, peers),
        flags(levels), flags(levels), flags(levels), flags(levels),
    ]
    return pl.pallas_call(
        functools.partial(layer_kernel, experts_here, share, (len(near), len(far), len(mixer_own))),
        in_specs=[vmem] * len(near) + [anywhere] * len(far),
        out_specs=vmem,
        out_shape=jax.ShapeDtypeStruct((owned, features), jnp.float32),
        scratch_shapes=[half(*array.shape) for array in far]
        + [half(owned, features), half(owned, features), full(seats, 8, 128)]
        + mixer_own + shared + mixer_flags + experts_own + experts_flags + [flags(len(far))],
        compiler_params=pltpu.CompilerParams(
            collective_id=0, has_side_effects=True, vmem_limit_bytes=67043328
        ),
        name="layer",
    )(*near, *far).astype(jnp.bfloat16)


def solution(mesh):
    in_specs = (
        P(("sp", "tp"), None),
        P("sp", "tp"),
        P("sp", "tp"),
        P("sp", "tp"),
        P("sp", "tp"),
        P(None, "tp"),
        P(None, "tp"),
        P(None, "tp"),
        P(None, "tp", "sp"),
        P(None, "tp"),
        P(None, "tp", "sp"),
        P("tp"),
        P("tp", None),
        P(),
        P("sp", None, "tp"),
        P("sp", None, "tp"),
        P("sp", "tp", None),
        P(("sp", "tp"), None),
        P(("sp", "tp"), None),
    )
    out_specs = P(("sp", "tp"), None)
    return jax.shard_map(
        per_device, mesh=mesh, in_specs=in_specs, out_specs=out_specs, check_vma=False
    )
```
